32 devices in a mesh: ep: 8 (over z, y), tp: 4 (over x, core).
Axes of the slice: x: 2, y: 2, z: 4, core: 2. Of those that a mesh axis runs over, the one named last changes fastest.
Arguments:
- tokens: bfloat16 [6144, 2048], P('ep', 'tp')
- norm_gain: float32 [2048], P('tp'), may hold values from 0.1 to 1.9
- routing: int32 [6144, 2], P('ep'), may hold values from 0 to 7, as said below
- route_weight: float32 [6144, 2], P('ep'), may hold values from 0.2 to 1
- w_gate: bfloat16 [8, 2048, 512], P('ep', 'tp'), may hold values from -0.125 to 0.125
- w_up: bfloat16 [8, 2048, 512], P('ep', 'tp'), may hold values from -0.125 to 0.125
- w_down: bfloat16 [8, 512, 2048], P('ep', None, 'tp'), may hold values from -0.25 to 0.25
- w_branch_in: bfloat16 [2048, 1024], P('ep', 'tp'), may hold values from -0.125 to 0.125
- w_branch_out: bfloat16 [1024, 2048], P('tp', 'ep'), may hold values from -0.1875 to 0.1875
- branch_gate: float32 [2048], P('tp'), may hold values from -3 to 3
Outputs:
- mixed: bfloat16 [6144, 2048], P('ep', 'tp')
The draws below stay inside these ranges and needn't reach their ends.
Inputs may be any that keep to these rules, and one draw needn't show every extreme that they name: `routing`: each row names two different experts of the same group; expert e belongs to group e // 2. Among the rows of one device (aligned blocks of 768 rows) no expert is named more than 384 times, and in every block all experts of one group are named exactly 384 times.
All inputs are finite; a program needn't handle non-finite values.
Results may differ from the reference program's by a relative error of at most 0.0069.
Values may be sent and summed in bfloat16 or wider, within the bound.
A program may use at most 128 MiB of HBM per device.

```python
import math
import jax
import jax.numpy as jnp
from jax import lax

D = 2048
FF = 512
BR = 1024
GROUPS = 4
TOK_DEV = 768
EXPERTS = 8
CAP = 384
TOKENS = 6144
N_EP = 8
N_TP = 4


def draw_tokens(key, part):
    first, second = jax.random.split(key, 2)
    base = jax.random.normal(first, (TOKENS, D), jnp.float32)
    scales = jnp.exp(jax.random.uniform(second, (N_TP,), jnp.float32, math.log(0.3), math.log(3.0)))
    values = base.reshape(TOKENS, N_TP, D // N_TP) * scales[None, :, None]
    return values.reshape(TOKENS, D).astype(jnp.bfloat16)


def draw_routing(key, part):
    per_group = EXPERTS // GROUPS
    half = TOK_DEV // 2

    def one_block(block):
        block_key = jax.random.fold_in(key, block)
        keys = jax.random.split(block_key, 3 + GROUPS)
        busiest = jax.random.randint(keys[0], (), 0, GROUPS)
        cuts = jax.random.randint(keys[1], (2,), 0, half + 1)
        lower = jnp.min(cuts)
        upper = jnp.max(cuts)
        others = jnp.stack([lower, upper - lower, half - upper])
        group_ids = jnp.arange(GROUPS, dtype=jnp.int32)
        other_place = jnp.clip(group_ids - (group_ids > busiest).astype(jnp.int32), 0, 2)
        counts = jnp.where(group_ids == busiest, half, others[other_place])
        ends = jnp.cumsum(counts)
        starts = ends - counts
        position = jnp.arange(TOK_DEV, dtype=jnp.int32)
        group = jnp.sum((position[:, None] >= ends[None, :]).astype(jnp.int32), axis=1)
        local = position - starts[group]
        orders = jnp.stack([jax.random.permutation(keys[3 + g], per_group) for g in range(GROUPS)]).astype(jnp.int32)
        offset = 1 + local // per_group % (per_group - 1)
        first = orders[group, local % per_group]
        second = orders[group, (local + offset) % per_group]
        paired = jnp.stack([group * per_group + first, group * per_group + second], axis=1)
        shuffle = jax.random.permutation(keys[2], TOK_DEV)
        return paired[shuffle]
    blocks = jax.vmap(one_block)(jnp.arange(N_EP, dtype=jnp.int32))
    return blocks.reshape(TOKENS, 2).astype(jnp.int32)


def levels(rng, shape, cuts, low, high):
    def one(dim, shards_of):
        heights = jax.random.uniform(jax.random.fold_in(jax.random.fold_in(rng, 6), dim), (shards_of,), jnp.float32, low / len(cuts), high / len(cuts))
        return jnp.repeat(jnp.exp(heights), shape[dim] // shards_of).reshape((-1,) + (1,) * (len(shape) - dim - 1))

    gain = one(*cuts[0])
    for cut in cuts[1:]:
        gain = gain * one(*cut)
    return gain


def normal_values(own_key, extent, spread, most, cuts=(), held_as=jnp.bfloat16):
    level = levels(own_key, extent, cuts, -0.22, 0.18) if cuts else 1.0
    array = jax.random.normal(own_key, extent, jnp.float32) * spread * level
    return jnp.minimum(jnp.maximum(array, -most), most).astype(held_as)


def setup_inputs(seed: int = 0) -> dict:
    splits = jax.random.split(jax.random.key(seed), 11)
    return {
        "tokens": draw_tokens(jax.random.fold_in(splits[10], 71), 0),
        "norm_gain": jnp.clip(1.0 + 0.18 * jax.random.normal(splits[1], (D,), jnp.float32), 0.1, 1.9),
        "routing": draw_routing(jax.random.fold_in(splits[10], 71), 0),
        "route_weight": jnp.clip(0.2 + 0.8 * jax.random.uniform(splits[3], (TOKENS, 2), jnp.float32) ** levels(splits[3], (TOKENS, 2), ((0, 8),), -0.2, 0.2), 0.2, 1.0),
        "w_gate": normal_values(splits[4], (EXPERTS, D, FF), D ** -0.5, 0.125, ((0, 8), (1, 4))),
        "w_up": normal_values(splits[5], (EXPERTS, D, FF), D ** -0.5, 0.125, ((0, 8), (1, 4))),
        "w_down": normal_values(splits[6], (EXPERTS, FF, D), FF ** -0.5, 0.25, ((0, 8), (2, 4))),
        "w_branch_in": normal_values(splits[7], (D, BR), D ** -0.5, 0.125, ((0, 8), (1, 4))),
        "w_branch_out": normal_values(splits[8], (BR, D), BR ** -0.5, 0.1875, ((0, 4), (1, 8))),
        "branch_gate": jnp.clip(jax.random.uniform(splits[9], (D,), jnp.float32, -3.0, 3.0) * levels(splits[9], (D,), ((0, 4),), -0.4, 0.0), -3.0, 3.0),
    }


epsilon = 1e-06

def slot_numbers(routing):
    flat_ids = routing.reshape(N_EP, TOK_DEV * 2)
    one_hot = (flat_ids[:, :, None] == jnp.arange(EXPERTS, dtype=jnp.int32)[None, None, :]).astype(jnp.int32)
    before = jnp.cumsum(one_hot, axis=1) - one_hot
    return lax.optimization_barrier(jnp.sum(before * one_hot, axis=2)).reshape(TOKENS, 2).astype(jnp.int32)

def expert(operands):
    inputs, gate_weight, up_weight, down_weight = operands
    gate_sum = jnp.dot(inputs, gate_weight, preferred_element_type=jnp.float32)
    up_sum = jnp.dot(inputs, up_weight, preferred_element_type=jnp.float32)
    hidden = (jax.nn.silu(gate_sum) * up_sum).astype(jnp.bfloat16)
    return jnp.dot(hidden, down_weight, preferred_element_type=jnp.float32).astype(jnp.bfloat16)

def reference(tokens, norm_gain, routing, route_weight, w_gate, w_up, w_down, w_branch_in, w_branch_out, branch_gate):
    floats = tokens.astype(jnp.float32)
    squares = lax.optimization_barrier(jnp.mean(floats * floats, axis=1, keepdims=True))
    normed = (floats * lax.rsqrt(squares + epsilon) * norm_gain).astype(jnp.bfloat16)
    source = (jnp.arange(TOKENS, dtype=jnp.int32) // TOK_DEV)[:, None]
    place = (source * CAP + slot_numbers(routing)).astype(jnp.int32)
    copies = jnp.broadcast_to(normed[:, None, :], (TOKENS, 2, D))
    buffer = jnp.zeros((EXPERTS, N_EP * CAP, D), jnp.bfloat16).at[routing, place].set(copies)
    outputs = lax.map(expert, (buffer, w_gate, w_up, w_down))
    picked = outputs[routing, place].astype(jnp.float32)
    routed = lax.optimization_barrier(jnp.sum(picked * route_weight[:, :, None], axis=1))
    branch_hidden = jax.nn.silu(jnp.dot(normed, w_branch_in, preferred_element_type=jnp.float32)).astype(jnp.bfloat16)
    branch = jnp.dot(branch_hidden, w_branch_out, preferred_element_type=jnp.float32).astype(jnp.bfloat16)
    return (routed + jax.nn.sigmoid(branch_gate) * branch.astype(jnp.float32)).astype(jnp.bfloat16)
```

```python
import functools

import jax
import jax.numpy as jnp
from jax import lax
from jax.experimental import pallas as pl
from jax.experimental.pallas import tpu as pltpu
from jax.sharding import PartitionSpec as P

GROUPS = 4


epsilon = 1e-06


def send_back(result):
    return lax.all_to_all(result, "ep", split_axis=0, concat_axis=0, tiled=True)


def body(
    tokens,
    norm_gain,
    routing,
    route_weight,
    w_gate,
    w_up,
    w_down,
    w_branch_in,
    w_branch_out,
    branch_gate,
):
    token_count, quarter = tokens.shape
    full_width = quarter * lax.axis_size("tp")
    floats = tokens.astype(jnp.float32)
    squares = lax.psum(jnp.sum(floats * floats, axis=1), "tp")
    normed = (floats * lax.rsqrt(squares[:, None] / full_width + epsilon) * norm_gain).astype(
        jnp.bfloat16
    )
    expert_count = lax.axis_size("ep") * w_gate.shape[0]
    capacity = token_count // (expert_count // GROUPS)
    flat_ids = routing.reshape(-1)
    one_hot = (flat_ids[:, None] == jnp.arange(expert_count, dtype=jnp.int32)[None, :]).astype(
        jnp.int32
    )
    before = jnp.cumsum(one_hot, axis=0) - one_hot
    position = flat_ids * capacity + jnp.sum(before * one_hot, axis=1)
    copies = jnp.repeat(normed, 2, axis=0)
    buffer = jnp.zeros((expert_count * capacity, quarter), jnp.bfloat16).at[position].set(copies)
    buffer = buffer.reshape(expert_count, capacity, quarter)
    gate_whole, up_whole, down_whole = (
        lax.all_gather(w_gate[0], "tp", axis=0, tiled=True),
        lax.all_gather(w_up[0], "tp", axis=0, tiled=True),
        lax.all_gather(w_down[0], "tp", axis=1, tiled=True),
    )
    row_split = lax.all_to_all(
        lax.all_to_all(buffer, "ep", split_axis=0, concat_axis=0, tiled=True),
        "tp",
        split_axis=0,
        concat_axis=2,
        tiled=True,
    )
    slot_rows = row_split.reshape(-1, row_split.shape[2])
    gate_sum = jnp.dot(slot_rows, gate_whole, preferred_element_type=jnp.float32)
    up_sum = jnp.dot(slot_rows, up_whole, preferred_element_type=jnp.float32)
    hidden = (jax.nn.silu(gate_sum) * up_sum).astype(jnp.bfloat16)
    result = jnp.dot(hidden, down_whole, preferred_element_type=jnp.float32).astype(jnp.bfloat16)
    feature_split = lax.all_to_all(
        result.reshape(row_split.shape), "tp", split_axis=2, concat_axis=0, tiled=True
    )
    returned = send_back(feature_split)
    picked = returned.reshape(expert_count * capacity, quarter)[position].reshape(
        token_count, 2, quarter
    )
    routed = jnp.sum(picked.astype(jnp.float32) * route_weight[:, :, None], axis=1)
    branch_tokens = lax.all_to_all(normed, "tp", split_axis=0, concat_axis=1, tiled=True)
    in_cols, out_rows = (
        lax.all_gather(w_branch_in, "tp", axis=1, tiled=True),
        lax.all_gather(w_branch_out, "tp", axis=0, tiled=True),
    )
    in_whole, out_whole = (
        lax.all_gather(in_cols, "ep", axis=0, tiled=True),
        lax.all_gather(out_rows, "ep", axis=1, tiled=True),
    )
    branch_hidden = jax.nn.silu(
        jnp.dot(branch_tokens, in_whole, preferred_element_type=jnp.float32)
    ).astype(jnp.bfloat16)
    branch_local = jnp.dot(branch_hidden, out_whole, preferred_element_type=jnp.float32).astype(
        jnp.bfloat16
    )
    branch = lax.all_to_all(branch_local, "tp", split_axis=1, concat_axis=0, tiled=True)
    return (routed + jax.nn.sigmoid(branch_gate) * branch.astype(jnp.float32)).astype(jnp.bfloat16)


BF16, F32 = jnp.bfloat16, jnp.float32
COPIES = 54
VMEM_LIMIT = 46 * 1024 * 1024


def dot(a, b):
    return jnp.dot(a, b, preferred_element_type=F32)


def dot_nt(a, b):
    return lax.dot_general(a, b, (((1,), (1,)), ((), ())), preferred_element_type=F32)


def silu(v):
    return v / (1.0 + jnp.exp(-v))


def pair_kernel(
    tokens_hbm,
    gain_hbm,
    routing_hbm,
    route_weight_hbm,
    w_gate,
    w_up,
    w_down,
    w_in,
    w_out,
    branch_gate_hbm,
    out,
    tokens,
    gain,
    routing,
    route_weight,
    branch_gate,
    gate_all,
    up_all,
    down_all,
    squares,
    scaled,
    branch_all,
    chosen,
    slots_out,
    slots,
    slots_s,
    scale_out,
    scale,
    scale_col,
    part_out,
    part_own,
    part_in,
    hidden,
    half_out,
    half_own,
    half_in,
    back_out,
    back,
    fold_out,
    fold_own,
    fold_in,
    cross_out,
    cross_in,
    branch_hidden,
    code_col,
    factor_col,
    load_sem,
    send_sem,
    recv_sem,
):
    ep, tp = lax.axis_index("ep"), lax.axis_index("tp")
    z, y, x, c = ep // 2, ep % 2, tp // 2, tp % 2
    token_count, quarter = tokens.shape
    ff = w_gate.shape[1]
    capacity = slots.shape[1]
    half = capacity // 2
    block = w_in.shape[0]

    def at(zz, yy, xx, cc):
        return (zz * 2 + yy, xx * 2 + cc)

    sibling = at(z, y, x, 1 - c)
    across = at(z, y, 1 - x, c)
    diagonal = at(z, y, 1 - x, 1 - c)
    pair = at(z, 1 - y, x, c)
    pair_user = at(z, 1 - y, x, y)
    pair_other = at(z, 1 - y, x, 1 - c)
    level = [z, z + 1 - 2 * (z % 2), (z + 2) % GROUPS, GROUPS - 1 - z]
    peer_of = [None] + [at(level[m], y, x, c) for m in range(1, GROUPS)]
    up = at((z + 1) % GROUPS, y, x, c)
    down = at((z + GROUPS - 1) % GROUPS, y, x, c)

    barrier = pltpu.get_barrier_semaphore()
    peers = [sibling, across, diagonal, pair, pair_other] + peer_of[1:]
    for peer in peers:
        pl.semaphore_signal(
            barrier, inc=1, device_id=peer, device_id_type=pl.DeviceIdType.MESH
        )

    loads = [
        pltpu.make_async_copy(source, target, load_sem.at[number])
        for number, (source, target) in enumerate(
            (
                (routing_hbm, routing),
                (tokens_hbm, tokens),
                (gain_hbm, gain),
                (route_weight_hbm, route_weight),
                (branch_gate_hbm, branch_gate),
                (w_in, branch_all.at[y, z, 0]),
                (w_out, branch_all.at[y, z, 1]),
            )
        )
    ]
    for load in loads:
        load.start()

    weights_of = ((w_gate, gate_all), (w_up, up_all), (w_down, down_all))

    def weight_load(k):
        source, target = weights_of[k]
        return pltpu.make_async_copy(source, target.at[c], load_sem.at[len(loads) + k])

    @pl.when(c == y)
    def _():
        for k in range(3):
            weight_load(k).start()

    loads[0].wait()
    ids = routing[0:1, :]
    group = lax.shift_right_logical(ids, 1)
    rows16 = lax.broadcasted_iota(jnp.int32, (16, token_count), 0)
    member = jnp.where(rows16 == group, 1.0, 0.0)
    earlier = jnp.where(
        lax.broadcasted_iota(jnp.int32, (token_count, token_count), 0)
        < lax.broadcasted_iota(jnp.int32, (token_count, token_count), 1),
        1.0,
        0.0,
    ).astype(BF16)
    before = dot(member.astype(BF16), earlier)
    place = jnp.sum(member * before, axis=0, keepdims=True)
    code = group.astype(F32) * capacity + place

    loads[1].wait()
    loads[2].wait()
    floats = tokens[...].astype(F32)
    scaled[0] = (floats * gain[...]).astype(BF16)
    exact = floats * floats
    high = exact.astype(BF16)
    low = (exact - high.astype(F32)).astype(BF16)
    ones = jnp.ones((16, quarter), BF16)
    squares[0] = (dot_nt(ones, high) + dot_nt(ones, low))[:8]

    slot_row = lax.broadcasted_iota(jnp.int32, (capacity, token_count), 0)

    def choose_rows(s):
        wanted = (slot_row + level[s] * capacity).astype(F32)
        chosen[s] = jnp.where(wanted == code, 1.0, 0.0).astype(BF16)
        rows = dot(chosen[s], scaled[0]).astype(BF16)
        if s == 0:
            slots[0] = rows
        else:
            slots_out[s] = rows

    choose_rows(2)

    pl.semaphore_wait(barrier, len(peers))

    started = {}

    def send(number, source, target, device):
        copy = pltpu.make_async_remote_copy(
            src_ref=source,
            dst_ref=target,
            send_sem=send_sem.at[number],
            recv_sem=recv_sem.at[number],
            device_id=device,
            device_id_type=pl.DeviceIdType.MESH,
        )
        copy.start()
        started[number] = copy

    def send_if(condition, number, source, target, device):
        copy = pltpu.make_async_remote_copy(
            src_ref=source,
            dst_ref=target,
            send_sem=send_sem.at[number],
            recv_sem=recv_sem.at[number],
            device_id=device,
            device_id_type=pl.DeviceIdType.MESH,
        )

        @pl.when(condition)
        def _():
            copy.start()

        started[number] = copy

    def arrived(number):
        started[number].wait_recv()

    def weight_copy(k, sem, device):
        source, target = weights_of[k]
        return pltpu.make_async_remote_copy(
            src_ref=source,
            dst_ref=target.at[c],
            send_sem=send_sem.at[2 * k + sem],
            recv_sem=recv_sem.at[2 * k + c],
            device_id=device,
            device_id_type=pl.DeviceIdType.MESH,
        )

    def send_slots(s):
        send(19 + s, slots_out.at[s], slots.at[s], peer_of[s])

    def send_slots_if(condition, s):
        send_if(condition, 19 + s, slots_out.at[s], slots.at[s], peer_of[s])

    def send_scale(s):
        send(22 + s, scale_out.at[s], scale.at[s], peer_of[s])

    def relay(hop, upward):
        number = (12 if upward else 47) + hop - 1
        held = z - (hop - 1) if upward else z + (hop - 1)
        came = z - hop if upward else z + hop
        held, came = (held + GROUPS) % GROUPS, (came + GROUPS) % GROUPS
        sends = (z <= GROUPS - 2) & (z >= hop - 1)
        gets = z >= hop
        if not upward:
            sends = (z >= 1) & (z <= GROUPS - hop)
            gets = z <= GROUPS - 1 - hop

        def copy(row):
            return pltpu.make_async_remote_copy(
                src_ref=branch_all.at[y, row],
                dst_ref=branch_all.at[y, row],
                send_sem=send_sem.at[number],
                recv_sem=recv_sem.at[number],
                device_id=up if upward else down,
                device_id_type=pl.DeviceIdType.MESH,
            )

        return sends, gets, lambda: copy(held), lambda: copy(came)

    def relay_start(hop):
        for upward in (True, False):
            sends, _, outgoing, _ = relay(hop, upward)

            @pl.when(sends)
            def _():
                outgoing().start()

    def relay_arrived(hop):
        for upward in (True, False):
            _, gets, _, incoming = relay(hop, upward)

            @pl.when(gets)
            def _():
                incoming().wait_recv()

    def relay_sent(hop):
        for upward in (True, False):
            sends, _, outgoing, _ = relay(hop, upward)

            @pl.when(sends)
            def _():
                outgoing().wait_send()

    send(7, squares.at[0], squares.at[2], across)
    send(8, squares.at[0], squares.at[3], diagonal)
    send(6, squares.at[0], squares.at[1], sibling)
    outer = (z == 0) | (z == GROUPS - 1)
    early = c == y
    send_slots(2)
    loads[5].wait()
    loads[6].wait()
    relay_start(1)
    send_if(c != y, 10, scaled.at[0], scaled.at[2], across)
    for k in range(3):
        weight_copy(k, 0, pair_user).start()

    @pl.when(c != y)
    def _():
        for k in range(3):
            weight_copy(k, 1, sibling).start()

    send(9, scaled.at[0], scaled.at[1], sibling)

    def weight_arrived(k):
        source, target = weights_of[k]

        def wait(h):
            pltpu.make_async_remote_copy(
                src_ref=source,
                dst_ref=target.at[h],
                send_sem=send_sem.at[2 * k],
                recv_sem=recv_sem.at[2 * k + h],
                device_id=sibling,
                device_id_type=pl.DeviceIdType.MESH,
            ).wait_recv()

        wait(1 - c)

        @pl.when(c != y)
        def _():
            wait(c)

        @pl.when(c == y)
        def _():
            weight_load(k).wait()

    def pair_send(m):
        rows = branch_all.at[y, level[m]]
        send(15 + m, rows, rows, pair)

    choose_rows(0)
    send(26, slots.at[0], slots_s.at[0], sibling)
    choose_rows(1)
    choose_rows(3)
    pair_send(0)

    loads[3].wait()
    loads[4].wait()
    first, second = route_weight[0:1, :], route_weight[1:2, :]
    even_first = (ids & 1) == 0
    for_even = jnp.where(even_first, first, second)
    for_odd = jnp.where(even_first, second, first)
    for number in (6, 7, 8):
        arrived(number)
    total = squares[0] + squares[1] + squares[2] + squares[3]
    factor = lax.rsqrt(total / (4 * quarter) + epsilon)
    factor_col[...] = jnp.transpose(factor)
    code_col[...] = jnp.transpose(jnp.broadcast_to(code, (8, token_count)))
    weights = jnp.where(
        rows16 == 0, for_even, jnp.where(rows16 == 1, for_odd, factor[0:1, :])
    )
    weights_high = weights.astype(BF16)
    weights_low = (weights - weights_high.astype(F32)).astype(BF16)
    for s in (2, 1, 3, 0):
        slot_weights = (dot_nt(weights_high, chosen[s]) + dot_nt(weights_low, chosen[s]))[:8]
        if s == 0:
            scale[0] = slot_weights
        else:
            scale_out[s] = slot_weights
            send_scale(s)
    send_slots_if(outer, 1)
    send_slots_if(outer, 3)

    def project(s, start, weights):
        own = slots[s, pl.ds(start, half), :]
        other = slots_s[s, pl.ds(start, half), :]
        return dot(own, weights[c]) + dot(other, weights[1 - c])

    mine = pl.multiple_of(x * half, half)
    theirs = pl.multiple_of((1 - x) * half, half)

    def forward(s):
        if s:
            arrived(19 + s)
            send(26 + s, slots.at[s], slots_s.at[s], sibling)

    sides = (slice(0, ff), slice(ff, 2 * ff))

    def stage_a(s):
        arrived(26 + s)
        for side, weights in zip(sides, (gate_all, up_all)):
            part_out[s, :, side] = project(s, theirs, weights).astype(BF16)
        send(30 + s, part_out.at[s], part_in.at[s], across)
        for side, weights in zip(sides, (gate_all, up_all)):
            part_own[s, :, side] = project(s, mine, weights)

    def stage_a_side(s, k):
        if k == 0:
            arrived(26 + s)
        side, weights = sides[k], (gate_all, up_all)[k]
        part_out[s, :, side] = project(s, theirs, weights).astype(BF16)
        number = 30 + s if k == 0 else 50 + s
        send(number, part_out.at[s, :, side], part_in.at[s, :, side], across)
        part_own[s, :, side] = project(s, mine, weights)

    def stage_b(s):
        if s:
            arrived(22 + s)
        scale_col[s] = jnp.transpose(scale[s])
        arrived(30 + s)
        if 50 + s in started:
            arrived(50 + s)
        rescale = scale_col[s, pl.ds(mine, half), 2:3]
        gate_sum = (part_own[s, :, :ff] + part_in[s, :, :ff].astype(F32)) * rescale
        up_sum = (part_own[s, :, ff:] + part_in[s, :, ff:].astype(F32)) * rescale
        hidden[s, pl.ds(mine, half), :] = (silu(gate_sum) * up_sum).astype(BF16)
        kept = hidden.at[s, pl.ds(mine, half), :]
        send(34 + s, kept, kept, across)

    def stage_c(s):
        arrived(34 + s)
        weight = jnp.where(c == 0, scale_col[s, :, 0:1], scale_col[s, :, 1:2])
        units = hidden[s]
        half_out[s] = (dot(units, down_all[1 - c]) * weight).astype(BF16)
        send(38 + s, half_out.at[s], half_in.at[s], sibling)
        half_own[s] = dot(units, down_all[c]) * weight

    def stage_d(s):
        arrived(38 + s)
        both = (half_own[s] + half_in[s].astype(F32)).astype(BF16)
        if s == 0:
            back[0] = both
        else:
            back_out[s] = both
            send(41 + s, back_out.at[s], back.at[s], peer_of[s])

    quarters = (tp, x * 2 + 1 - c, (1 - x) * 2 + c, (1 - x) * 2 + 1 - c)

    def branch_first():
        sums = jnp.zeros((token_count, block), F32)
        for k, q in enumerate(quarters):
            sums = sums + dot(scaled[k, :, :block], branch_all[0, q, 0])
            sums = sums + dot(scaled[k, :, block:], branch_all[1, q, 0])
        branch_hidden[...] = silu(sums * factor_col[:, 0:1]).astype(BF16)

    def branch_part(q, side):
        return dot(branch_hidden[...], branch_all[side, q, 1])

    def branch_fold():
        for side in range(2):
            columns = slice(side * block, (side + 1) * block)
            fold_out[0, :, columns] = branch_part(quarters[1], side).astype(BF16)
            fold_out[1, :, columns] = branch_part(quarters[3], side).astype(BF16)
        send(45, fold_out, fold_in, sibling)

    def branch_cross():
        arrived(45)
        for side in range(2):
            columns = slice(side * block, (side + 1) * block)
            cross_out[:, columns] = (
                branch_part(quarters[2], side) + fold_in[1, :, columns].astype(F32)
            ).astype(BF16)
        send(46, cross_out, cross_in, across)

    def branch_own():
        for side in range(2):
            columns = slice(side * block, (side + 1) * block)
            fold_own[:, columns] = branch_part(quarters[0], side) + fold_in[
                0, :, columns
            ].astype(F32)

    slot_lane = lax.broadcasted_iota(jnp.int32, (token_count, capacity), 1)

    def restore(s):
        if s:
            arrived(41 + s)
        wanted = (slot_lane + level[s] * capacity).astype(F32)
        choose = jnp.where(wanted == code_col[:, 0:1], 1.0, 0.0).astype(BF16)
        return dot(choose, back[s])

    weight_arrived(0)
    stage_a_side(0, 0)
    weight_arrived(1)
    stage_a_side(0, 1)
    send_if(early, 10, scaled.at[0], scaled.at[2], across)
    forward(2)
    send_slots_if(~outer, 3)
    send_slots_if(~outer, 1)
    stage_a(2)
    stage_b(0)
    relay_arrived(1)
    relay_start(2)
    pair_send(1)
    arrived(10)
    send(11, scaled.at[2], scaled.at[3], sibling)
    forward(1)
    stage_b(2)
    weight_arrived(2)
    stage_c(0)
    stage_d(0)
    forward(3)
    stage_a(3)
    stage_c(2)
    stage_d(2)
    relay_arrived(2)
    relay_start(3)
    pair_send(2)
    stage_a_side(1, 0)
    stage_b(3)
    stage_a_side(1, 1)
    relay_arrived(3)
    pair_send(3)
    stage_c(3)
    stage_d(3)
    arrived(9)
    arrived(11)
    for m in range(GROUPS):
        arrived(15 + m)
    branch_first()
    branch_fold()
    stage_b(1)
    branch_cross()
    branch_own()
    stage_c(1)
    stage_d(1)

    half_own_sum = restore(0)
    for s in (2, 3, 1):
        half_own_sum = half_own_sum + restore(s)
    arrived(46)
    branch = fold_own[...] + cross_in[...].astype(F32)
    gate = 1.0 / (1.0 + jnp.exp(-branch_gate[...]))
    out[...] = (half_own_sum + gate * branch).astype(BF16)
    for copy in started.values():
        copy.wait_send()
    for hop in range(1, GROUPS):
        relay_sent(hop)
    for k in range(3):
        weight_copy(k, 0, pair_user).wait_send()

    @pl.when(c != y)
    def _():
        for k in range(3):
            weight_copy(k, 1, sibling).wait_send()


def pair_body(
    tokens,
    norm_gain,
    routing,
    route_weight,
    w_gate,
    w_up,
    w_down,
    w_branch_in,
    w_branch_out,
    branch_gate,
):
    count, quarter = tokens.shape
    ff = w_gate.shape[2]
    block = w_branch_in.shape[0]
    cap = count // 2
    half = cap // 2
    vmem = pltpu.VMEM
    rows = (GROUPS, cap, quarter)
    scratch = [
        vmem((count, quarter), BF16),
        vmem((1, quarter), F32),
        vmem((2, count), jnp.int32),
        vmem((2, count), F32),
        vmem((1, quarter), F32),
        vmem((2, quarter, ff), BF16),
        vmem((2, quarter, ff), BF16),
        vmem((2, ff, quarter), BF16),
        vmem((4, 8, count), F32),
        vmem((4, count, quarter), BF16),
        vmem((2, GROUPS, 2, block, block), BF16),
        vmem((GROUPS, cap, count), BF16),
        vmem(rows, BF16),
        vmem(rows, BF16),
        vmem(rows, BF16),
        vmem((GROUPS, 8, cap), F32),
        vmem((GROUPS, 8, cap), F32),
        vmem((GROUPS, cap, 8), F32),
        vmem((GROUPS, half, 2 * ff), BF16),
        vmem((GROUPS, half, 2 * ff), F32),
        vmem((GROUPS, half, 2 * ff), BF16),
        vmem((GROUPS, cap, ff), BF16),
        vmem(rows, BF16),
        vmem(rows, F32),
        vmem(rows, BF16),
        vmem(rows, BF16),
        vmem(rows, BF16),
        vmem((2, count, quarter), BF16),
        vmem((count, quarter), F32),
        vmem((2, count, quarter), BF16),
        vmem((count, quarter), BF16),
        vmem((count, quarter), BF16),
        vmem((count, block), BF16),
        vmem((count, 8), F32),
        vmem((count, 8), F32),
        pltpu.SemaphoreType.DMA((10,)),
        pltpu.SemaphoreType.DMA((COPIES,)),
        pltpu.SemaphoreType.DMA((COPIES,)),
    ]
    return pl.pallas_call(
        pair_kernel,
        out_shape=pltpu.VMEM((count, quarter), BF16),
        in_specs=[pl.BlockSpec(memory_space=pltpu.HBM)] * 10,
        out_specs=pl.BlockSpec(memory_space=vmem),
        scratch_shapes=scratch,
        compiler_params=pltpu.CompilerParams(
            collective_id=0, has_side_effects=True, vmem_limit_bytes=VMEM_LIMIT
        ),
    )(
        *(
            pltpu.with_memory_space_constraint(operand, pltpu.HBM)
            for operand in (
                tokens,
                norm_gain[None, :],
                routing.T,
                route_weight.T,
                w_gate[0],
                w_up[0],
                w_down[0],
                w_branch_in,
                w_branch_out,
                branch_gate[None, :],
            )
        )
    )


def solution(mesh):
    return jax.shard_map(
        pair_body if mesh.shape["ep"] == 2 * GROUPS and mesh.shape["tp"] == 4 else body,
        mesh=mesh,
        in_specs=(
            P("ep", "tp"),
            P("tp"),
            P("ep", None),
            P("ep", None),
            P("ep", "tp", None),
            P("ep", "tp", None),
            P("ep", None, "tp"),
            P("ep", "tp"),
            P("tp", "ep"),
            P("tp"),
        ),
        out_specs=P("ep", "tp"),
        check_vma=False,
    )
```

```python
import functools

import jax
import jax.numpy as jnp
from jax import lax
from jax.experimental import pallas as pl
from jax.experimental.pallas import tpu as pltpu
from jax.sharding import PartitionSpec as P

GROUPS = 4


epsilon = 1e-06


def send_back(result):
    return lax.all_to_all(result, "ep", split_axis=0, concat_axis=0, tiled=True)


def body(
    tokens,
    norm_gain,
    routing,
    route_weight,
    w_gate,
    w_up,
    w_down,
    w_branch_in,
    w_branch_out,
    branch_gate,
):
    token_count, quarter = tokens.shape
    full_width = quarter * lax.axis_size("tp")
    floats = tokens.astype(jnp.float32)
    squares = lax.psum(jnp.sum(floats * floats, axis=1), "tp")
    normed = (floats * lax.rsqrt(squares[:, None] / full_width + epsilon) * norm_gain).astype(
        jnp.bfloat16
    )
    expert_count = lax.axis_size("ep") * w_gate.shape[0]
    capacity = token_count // (expert_count // GROUPS)
    flat_ids = routing.reshape(-1)
    one_hot = (flat_ids[:, None] == jnp.arange(expert_count, dtype=jnp.int32)[None, :]).astype(
        jnp.int32
    )
    before = jnp.cumsum(one_hot, axis=0) - one_hot
    position = flat_ids * capacity + jnp.sum(before * one_hot, axis=1)
    copies = jnp.repeat(normed, 2, axis=0)
    buffer = jnp.zeros((expert_count * capacity, quarter), jnp.bfloat16).at[position].set(copies)
    buffer = buffer.reshape(expert_count, capacity, quarter)
    gate_whole, up_whole, down_whole = (
        lax.all_gather(w_gate[0], "tp", axis=0, tiled=True),
        lax.all_gather(w_up[0], "tp", axis=0, tiled=True),
        lax.all_gather(w_down[0], "tp", axis=1, tiled=True),
    )
    row_split = lax.all_to_all(
        lax.all_to_all(buffer, "ep", split_axis=0, concat_axis=0, tiled=True),
        "tp",
        split_axis=0,
        concat_axis=2,
        tiled=True,
    )
    slot_rows = row_split.reshape(-1, row_split.shape[2])
    gate_sum = jnp.dot(slot_rows, gate_whole, preferred_element_type=jnp.float32)
    up_sum = jnp.dot(slot_rows, up_whole, preferred_element_type=jnp.float32)
    hidden = (jax.nn.silu(gate_sum) * up_sum).astype(jnp.bfloat16)
    result = jnp.dot(hidden, down_whole, preferred_element_type=jnp.float32).astype(jnp.bfloat16)
    feature_split = lax.all_to_all(
        result.reshape(row_split.shape), "tp", split_axis=2, concat_axis=0, tiled=True
    )
    returned = send_back(feature_split)
    picked = returned.reshape(expert_count * capacity, quarter)[position].reshape(
        token_count, 2, quarter
    )
    routed = jnp.sum(picked.astype(jnp.float32) * route_weight[:, :, None], axis=1)
    branch_tokens = lax.all_to_all(normed, "tp", split_axis=0, concat_axis=1, tiled=True)
    in_cols, out_rows = (
        lax.all_gather(w_branch_in, "tp", axis=1, tiled=True),
        lax.all_gather(w_branch_out, "tp", axis=0, tiled=True),
    )
    in_whole, out_whole = (
        lax.all_gather(in_cols, "ep", axis=0, tiled=True),
        lax.all_gather(out_rows, "ep", axis=1, tiled=True),
    )
    branch_hidden = jax.nn.silu(
        jnp.dot(branch_tokens, in_whole, preferred_element_type=jnp.float32)
    ).astype(jnp.bfloat16)
    branch_local = jnp.dot(branch_hidden, out_whole, preferred_element_type=jnp.float32).astype(
        jnp.bfloat16
    )
    branch = lax.all_to_all(branch_local, "tp", split_axis=1, concat_axis=0, tiled=True)
    return (routed + jax.nn.sigmoid(branch_gate) * branch.astype(jnp.float32)).astype(jnp.bfloat16)


BF16, F32 = jnp.bfloat16, jnp.float32
COPIES = 61
VMEM_LIMIT = 46 * 1024 * 1024


def dot(a, b):
    return jnp.dot(a, b, preferred_element_type=F32)


def dot_nt(a, b):
    return lax.dot_general(a, b, (((1,), (1,)), ((), ())), preferred_element_type=F32)


def silu(v):
    return v / (1.0 + jnp.exp(-v))


def pair_kernel(
    tokens_hbm,
    gain_hbm,
    routing_hbm,
    route_weight_hbm,
    w_gate,
    w_up,
    w_down,
    w_in,
    w_out,
    branch_gate_hbm,
    out,
    tokens,
    gain,
    routing,
    route_weight,
    branch_gate,
    gate_all,
    up_all,
    down_all,
    squares,
    scaled,
    branch_all,
    chosen,
    slots_out,
    slots,
    slots_s,
    scale_out,
    scale,
    scale_col,
    part_out,
    part_own,
    part_in,
    hidden,
    half_out,
    half_own,
    half_in,
    back_out,
    back,
    fold_out,
    fold_own,
    fold_in,
    cross_out,
    cross_in,
    branch_hidden,
    branch_acc,
    code_col,
    factor_col,
    load_sem,
    send_sem,
    recv_sem,
):
    ep, tp = lax.axis_index("ep"), lax.axis_index("tp")
    z, y, x, c = ep // 2, ep % 2, tp // 2, tp % 2
    token_count, quarter = tokens.shape
    ff = w_gate.shape[1]
    capacity = slots.shape[1]
    half = capacity // 2
    block = w_in.shape[0]

    def at(zz, yy, xx, cc):
        return (zz * 2 + yy, xx * 2 + cc)

    sibling = at(z, y, x, 1 - c)
    across = at(z, y, 1 - x, c)
    diagonal = at(z, y, 1 - x, 1 - c)
    pair = at(z, 1 - y, x, c)
    pair_user = at(z, 1 - y, x, y)
    pair_other = at(z, 1 - y, x, 1 - c)
    level = [z, z + 1 - 2 * (z % 2), (z + 2) % GROUPS, GROUPS - 1 - z]
    peer_of = [None] + [at(level[m], y, x, c) for m in range(1, GROUPS)]
    up = at((z + 1) % GROUPS, y, x, c)
    down = at((z + GROUPS - 1) % GROUPS, y, x, c)

    barrier = pltpu.get_barrier_semaphore()
    peers = [sibling, across, diagonal, pair, pair_other] + peer_of[1:]
    for peer in peers:
        pl.semaphore_signal(
            barrier, inc=1, device_id=peer, device_id_type=pl.DeviceIdType.MESH
        )

    loads = [
        pltpu.make_async_copy(source, target, load_sem.at[number])
        for number, (source, target) in enumerate(
            (
                (routing_hbm, routing),
                (tokens_hbm, tokens),
                (gain_hbm, gain),
                (route_weight_hbm, route_weight),
                (branch_gate_hbm, branch_gate),
                (w_in, branch_all.at[y, z, 0]),
                (w_out, branch_all.at[y, z, 1]),
            )
        )
    ]
    for load in loads:
        load.start()

    weights_of = ((w_gate, gate_all), (w_up, up_all), (w_down, down_all))

    def weight_load(k):
        source, target = weights_of[k]
        return pltpu.make_async_copy(source, target.at[c], load_sem.at[len(loads) + k])

    @pl.when(c == y)
    def _():
        for k in range(3):
            weight_load(k).start()

    loads[0].wait()
    ids = routing[0:1, :]
    group = lax.shift_right_logical(ids, 1)
    rows16 = lax.broadcasted_iota(jnp.int32, (16, token_count), 0)
    member = jnp.where(rows16 == group, 1.0, 0.0)
    earlier = jnp.where(
        lax.broadcasted_iota(jnp.int32, (token_count, token_count), 0)
        < lax.broadcasted_iota(jnp.int32, (token_count, token_count), 1),
        1.0,
        0.0,
    ).astype(BF16)
    before = dot(member.astype(BF16), earlier)
    place = jnp.sum(member * before, axis=0, keepdims=True)
    code = group.astype(F32) * capacity + place

    loads[1].wait()
    loads[2].wait()
    floats = tokens[...].astype(F32)
    scaled[0] = (floats * gain[...]).astype(BF16)
    exact = floats * floats
    high = exact.astype(BF16)
    low = (exact - high.astype(F32)).astype(BF16)
    ones = jnp.ones((16, quarter), BF16)
    squares[0] = (dot_nt(ones, high) + dot_nt(ones, low))[:8]

    slot_row = lax.broadcasted_iota(jnp.int32, (capacity, token_count), 0)

    def choose_rows(s, where, target):
        wanted = (slot_row + where * capacity).astype(F32)
        chosen[s] = jnp.where(wanted == code, 1.0, 0.0).astype(BF16)
        target[s] = dot(chosen[s], scaled[0]).astype(BF16)

    outer = (z == 0) | (z == GROUPS - 1)
    near = jnp.where(outer, 1, 2)
    choose_rows(near, jnp.where(outer, level[1], level[2]), slots_out)

    pl.semaphore_wait(barrier, len(peers))

    started = {}

    def is_own(s):
        return isinstance(s, int) and s == 0

    def key_of(number):
        return number if isinstance(number, int) else ("dynamic", len(started))

    def wait_for(number, target):
        pltpu.make_async_remote_copy(
            src_ref=target,
            dst_ref=target,
            send_sem=send_sem.at[number],
            recv_sem=recv_sem.at[number],
            device_id=sibling,
            device_id_type=pl.DeviceIdType.MESH,
        ).wait_recv()

    def send(number, source, target, device):
        copy = pltpu.make_async_remote_copy(
            src_ref=source,
            dst_ref=target,
            send_sem=send_sem.at[number],
            recv_sem=recv_sem.at[number],
            device_id=device,
            device_id_type=pl.DeviceIdType.MESH,
        )
        copy.start()
        started[key_of(number)] = copy

    def send_if(condition, number, source, target, device):
        copy = pltpu.make_async_remote_copy(
            src_ref=source,
            dst_ref=target,
            send_sem=send_sem.at[number],
            recv_sem=recv_sem.at[number],
            device_id=device,
            device_id_type=pl.DeviceIdType.MESH,
        )

        @pl.when(condition)
        def _():
            copy.start()

        started[number] = copy

    def arrived(number):
        started[number].wait_recv()

    def weight_copy(k, sem, device):
        source, target = weights_of[k]
        return pltpu.make_async_remote_copy(
            src_ref=source,
            dst_ref=target.at[c],
            send_sem=send_sem.at[2 * k + sem],
            recv_sem=recv_sem.at[2 * k + c],
            device_id=device,
            device_id_type=pl.DeviceIdType.MESH,
        )

    def send_slots(s):
        send(19 + s, slots_out.at[s], slots.at[s], peer_of[s])

    def send_slots_if(condition, s):
        send_if(condition, 19 + s, slots_out.at[s], slots.at[s], peer_of[s])

    def send_scale(s):
        send(22 + s, scale_out.at[s], scale.at[s], peer_of[s])

    def relay(hop, upward):
        number = (12 if upward else 47) + hop - 1
        held = z - (hop - 1) if upward else z + (hop - 1)
        came = z - hop if upward else z + hop
        held, came = (held + GROUPS) % GROUPS, (came + GROUPS) % GROUPS
        sends = (z <= GROUPS - 2) & (z >= hop - 1)
        gets = z >= hop
        if not upward:
            sends = (z >= 1) & (z <= GROUPS - hop)
            gets = z <= GROUPS - 1 - hop

        def copy(row):
            return pltpu.make_async_remote_copy(
                src_ref=branch_all.at[y, row],
                dst_ref=branch_all.at[y, row],
                send_sem=send_sem.at[number],
                recv_sem=recv_sem.at[number],
                device_id=up if upward else down,
                device_id_type=pl.DeviceIdType.MESH,
            )

        return sends, gets, lambda: copy(held), lambda: copy(came)

    def relay_start(hop):
        for upward in (True, False):
            sends, _, outgoing, _ = relay(hop, upward)

            @pl.when(sends)
            def _():
                outgoing().start()

    def relay_arrived(hop):
        for upward in (True, False):
            _, gets, _, incoming = relay(hop, upward)

            @pl.when(gets)
            def _():
                incoming().wait_recv()

    def relay_sent(hop):
        for upward in (True, False):
            sends, _, outgoing, _ = relay(hop, upward)

            @pl.when(sends)
            def _():
                outgoing().wait_send()

    send(7, squares.at[0], squares.at[2], across)
    send(8, squares.at[0], squares.at[3], diagonal)
    send(6, squares.at[0], squares.at[1], sibling)
    early = c == y
    send_slots_if(outer, 1)
    send_slots_if(~outer, 2)
    part_rows = token_count // 2
    first_rows, last_rows = pl.ds(0, part_rows), pl.ds(part_rows, part_rows)

    def send_tokens(number, rows):
        return number, scaled.at[0, rows], scaled.at[2, rows], across

    send(*send_tokens(10, first_rows))
    send_if(~early, *send_tokens(57, last_rows))
    for k in range(3):
        weight_copy(k, 0, pair_user).start()

    @pl.when(c != y)
    def _():
        for k in range(3):
            weight_copy(k, 1, sibling).start()

    choose_rows(3 - near, jnp.where(outer, level[2], level[1]), slots_out)
    send_slots_if(outer, 2)
    loads[5].wait()
    loads[6].wait()
    relay_start(1)
    send(9, scaled.at[0], scaled.at[1], sibling)

    def weight_arrived(k):
        source, target = weights_of[k]

        def wait(h):
            pltpu.make_async_remote_copy(
                src_ref=source,
                dst_ref=target.at[h],
                send_sem=send_sem.at[2 * k],
                recv_sem=recv_sem.at[2 * k + h],
                device_id=sibling,
                device_id_type=pl.DeviceIdType.MESH,
            ).wait_recv()

        wait(1 - c)

        @pl.when(c != y)
        def _():
            wait(c)

        @pl.when(c == y)
        def _():
            weight_load(k).wait()

    def pair_send(m):
        rows = branch_all.at[y, level[m]]
        send(15 + m, rows, rows, pair)

    choose_rows(0, level[0], slots)
    send(26, slots.at[0], slots_s.at[0], sibling)
    choose_rows(3, level[3], slots_out)
    pair_send(0)

    loads[3].wait()
    loads[4].wait()
    first, second = route_weight[0:1, :], route_weight[1:2, :]
    even_first = (ids & 1) == 0
    for_even = jnp.where(even_first, first, second)
    for_odd = jnp.where(even_first, second, first)
    for number in (6, 7, 8):
        arrived(number)
    total = squares[0] + squares[1] + squares[2] + squares[3]
    factor = lax.rsqrt(total / (4 * quarter) + epsilon)
    factor_col[...] = jnp.transpose(factor)
    code_col[...] = jnp.transpose(jnp.broadcast_to(code, (8, token_count)))
    weights = jnp.where(
        rows16 == 0, for_even, jnp.where(rows16 == 1, for_odd, factor[0:1, :])
    )
    weights_high = weights.astype(BF16)
    weights_low = (weights - weights_high.astype(F32)).astype(BF16)
    for s in (2, 3, 1, 0):
        slot_weights = (dot_nt(weights_high, chosen[s]) + dot_nt(weights_low, chosen[s]))[:8]
        if s == 0:
            scale[0] = slot_weights
        else:
            scale_out[s] = slot_weights
            send_scale(s)
    send_slots_if(outer, 3)

    def project(s, start, weights):
        own = slots[s, pl.ds(start, half), :]
        other = slots_s[s, pl.ds(start, half), :]
        return dot(own, weights[c]) + dot(other, weights[1 - c])

    mine = pl.multiple_of(x * half, half)
    theirs = pl.multiple_of((1 - x) * half, half)

    def forward(s):
        wait_for(19 + s, slots.at[s])
        send(26 + s, slots.at[s], slots_s.at[s], sibling)

    sides = (slice(0, ff), slice(ff, 2 * ff))

    def stage_a(s):
        wait_for(26 + s, slots_s.at[s])
        for side, weights in zip(sides, (gate_all, up_all)):
            part_out[s, :, side] = project(s, theirs, weights).astype(BF16)
        send(30 + s, part_out.at[s], part_in.at[s], across)
        for side, weights in zip(sides, (gate_all, up_all)):
            part_own[s, :, side] = project(s, mine, weights)

    def stage_a_up_if(condition):
        number, side = 50, sides[1]
        copy = pltpu.make_async_remote_copy(
            src_ref=part_out.at[0, :, side],
            dst_ref=part_in.at[0, :, side],
            send_sem=send_sem.at[number],
            recv_sem=recv_sem.at[number],
            device_id=across,
            device_id_type=pl.DeviceIdType.MESH,
        )
        started[number] = copy

        @pl.when(condition)
        def _():
            part_out[0, :, side] = project(0, theirs, up_all).astype(BF16)
            copy.start()
            part_own[0, :, side] = project(0, mine, up_all)

    def stage_a_side(s, k):
        if k == 0:
            wait_for(26 + s, slots_s.at[s])
        side, weights = sides[k], (gate_all, up_all)[k]
        part_out[s, :, side] = project(s, theirs, weights).astype(BF16)
        number = 30 + s if k == 0 else 50 + s
        send(number, part_out.at[s, :, side], part_in.at[s, :, side], across)
        part_own[s, :, side] = project(s, mine, weights)

    def stage_b(s, sided=False):
        if not is_own(s):
            wait_for(22 + s, scale.at[s])
        scale_col[s] = jnp.transpose(scale[s])
        if is_own(s) or sided:
            wait_for(30 + s, part_in.at[s, :, sides[0]])
            wait_for(50 + s, part_in.at[s, :, sides[1]])
        else:
            wait_for(30 + s, part_in.at[s])
        rescale = scale_col[s, pl.ds(mine, half), 2:3]
        gate_sum = (part_own[s, :, :ff] + part_in[s, :, :ff].astype(F32)) * rescale
        up_sum = (part_own[s, :, ff:] + part_in[s, :, ff:].astype(F32)) * rescale
        hidden[s, pl.ds(mine, half), :] = (silu(gate_sum) * up_sum).astype(BF16)
        kept = hidden.at[s, pl.ds(mine, half), :]
        send(34 + s, kept, kept, across)

    def stage_c(s):
        wait_for(34 + s, hidden.at[s, pl.ds(theirs, half), :])
        weight = jnp.where(c == 0, scale_col[s, :, 0:1], scale_col[s, :, 1:2])
        units = hidden[s]
        half_out[s] = (dot(units, down_all[1 - c]) * weight).astype(BF16)
        send(38 + s, half_out.at[s], half_in.at[s], sibling)
        half_own[s] = dot(units, down_all[c]) * weight

    def stage_d(s):
        wait_for(38 + s, half_in.at[s])
        both = (half_own[s] + half_in[s].astype(F32)).astype(BF16)
        if is_own(s):
            back[0] = both
        else:
            back_out[s] = both
            zone = level[s] if isinstance(s, int) else jnp.where(s == 1, level[1], level[3])
            send(41 + s, back_out.at[s], back.at[s], at(zone, y, x, c))

    quarters = (tp, x * 2 + 1 - c, (1 - x) * 2 + c, (1 - x) * 2 + 1 - c)

    def branch_sum(members, first=False, last=False):
        sums = jnp.zeros((token_count, block), F32) if first else branch_acc[...]
        for m in members:
            wait_for(15 + m, branch_all.at[1 - y, level[m]])
            q = level[m]
            k = (x + q // 2) % 2 * 2 + (c + q) % 2
            sums = sums + dot(scaled[k, :, :block], branch_all[0, q, 0])
            sums = sums + dot(scaled[k, :, block:], branch_all[1, q, 0])
        if last:
            branch_hidden[...] = silu(sums * factor_col[:, 0:1]).astype(BF16)
        else:
            branch_acc[...] = sums

    def branch_part(q, side):
        return dot(branch_hidden[...], branch_all[side, q, 1])

    left, right = slice(0, block), slice(block, 2 * block)

    def branch_fold():
        for number, side, columns in ((54, 0, left), (55, 1, right)):
            fold_out[1, :, columns] = branch_part(quarters[3], side).astype(BF16)
            send(number, fold_out.at[1, :, columns], fold_in.at[1, :, columns], sibling)

    def branch_fold_own():
        for side, columns in ((0, left), (1, right)):
            fold_out[0, :, columns] = branch_part(quarters[1], side).astype(BF16)
        send(58, fold_out.at[0], fold_in.at[0], sibling)

    def branch_cross(number, side, rows):
        columns = (left, right)[side]
        cross_out[rows, columns] = (
            dot(branch_hidden[rows], branch_all[side, quarters[2], 1])
            + fold_in[1, rows, columns].astype(F32)
        ).astype(BF16)
        send(number, cross_out.at[rows, columns], cross_in.at[rows, columns], across)

    def branch_own():
        arrived(58)
        for side in range(2):
            columns = slice(side * block, (side + 1) * block)
            fold_own[:, columns] = branch_part(quarters[0], side) + fold_in[
                0, :, columns
            ].astype(F32)

    slot_lane = lax.broadcasted_iota(jnp.int32, (token_count, capacity), 1)

    def restore(s):
        if s:
            wait_for(41 + s, back.at[s])
        wanted = (slot_lane + level[s] * capacity).astype(F32)
        choose = jnp.where(wanted == code_col[:, 0:1], 1.0, 0.0).astype(BF16)
        return dot(choose, back[s])

    first = jnp.where(outer, 3, 1)
    last = 4 - first
    weight_arrived(0)
    stage_a_side(0, 0)

    @pl.when(early)
    def _():
        weight_arrived(1)

    stage_a_up_if(early)
    send_if(early & ~outer, *send_tokens(57, last_rows))
    forward(2)
    send_slots_if(~outer, 1)
    stage_a_side(2, 0)

    @pl.when(~early)
    def _():
        weight_arrived(1)

    stage_a_side(2, 1)
    send_if(early & outer, *send_tokens(57, last_rows))
    stage_a_up_if(~early)
    relay_arrived(1)
    relay_start(2)
    send_slots_if(~outer, 3)
    pair_send(1)
    stage_b(2, True)
    stage_b(0)
    forward(first)
    stage_a_side(first, 0)
    stage_a_side(first, 1)
    weight_arrived(2)
    stage_c(2)
    relay_arrived(2)
    relay_start(3)
    pair_send(2)
    stage_c(0)
    stage_d(0)
    arrived(10)
    arrived(57)
    send(11, scaled.at[2], scaled.at[3], sibling)
    forward(last)
    stage_d(2)
    stage_a_side(last, 0)
    relay_arrived(3)
    pair_send(3)
    stage_b(first, True)
    stage_a_side(last, 1)
    arrived(9)
    arrived(11)
    branch_sum((0, 1, 2), first=True)
    branch_sum((3,), last=True)
    branch_fold()
    arrived(54)
    branch_cross(46, 0, slice(0, capacity))
    stage_c(first)
    stage_d(first)
    stage_b(last, True)
    branch_cross(59, 0, slice(capacity, token_count))
    arrived(55)
    branch_cross(60, 1, slice(0, token_count))
    branch_fold_own()
    stage_c(last)
    stage_d(last)
    branch_own()

    half_own_sum = restore(0)
    half_own_sum = half_own_sum + restore(2)
    half_own_sum = half_own_sum + restore(3)
    half_own_sum = half_own_sum + restore(1)
    arrived(46)
    arrived(59)
    arrived(60)
    branch = fold_own[...] + cross_in[...].astype(F32)
    gate = 1.0 / (1.0 + jnp.exp(-branch_gate[...]))
    out[...] = (half_own_sum + gate * branch).astype(BF16)
    for copy in started.values():
        copy.wait_send()
    for hop in range(1, GROUPS):
        relay_sent(hop)
    for k in range(3):
        weight_copy(k, 0, pair_user).wait_send()

    @pl.when(c != y)
    def _():
        for k in range(3):
            weight_copy(k, 1, sibling).wait_send()


def pair_body(
    tokens,
    norm_gain,
    routing,
    route_weight,
    w_gate,
    w_up,
    w_down,
    w_branch_in,
    w_branch_out,
    branch_gate,
):
    count, quarter = tokens.shape
    ff = w_gate.shape[2]
    block = w_branch_in.shape[0]
    cap = count // 2
    half = cap // 2
    vmem = pltpu.VMEM
    rows = (GROUPS, cap, quarter)
    scratch = [
        vmem((count, quarter), BF16),
        vmem((1, quarter), F32),
        vmem((2, count), jnp.int32),
        vmem((2, count), F32),
        vmem((1, quarter), F32),
        vmem((2, quarter, ff), BF16),
        vmem((2, quarter, ff), BF16),
        vmem((2, ff, quarter), BF16),
        vmem((4, 8, count), F32),
        vmem((4, count, quarter), BF16),
        vmem((2, GROUPS, 2, block, block), BF16),
        vmem((GROUPS, cap, count), BF16),
        vmem(rows, BF16),
        vmem(rows, BF16),
        vmem(rows, BF16),
        vmem((GROUPS, 8, cap), F32),
        vmem((GROUPS, 8, cap), F32),
        vmem((GROUPS, cap, 8), F32),
        vmem((GROUPS, half, 2 * ff), BF16),
        vmem((GROUPS, half, 2 * ff), F32),
        vmem((GROUPS, half, 2 * ff), BF16),
        vmem((GROUPS, cap, ff), BF16),
        vmem(rows, BF16),
        vmem(rows, F32),
        vmem(rows, BF16),
        vmem(rows, BF16),
        vmem(rows, BF16),
        vmem((2, count, quarter), BF16),
        vmem((count, quarter), F32),
        vmem((2, count, quarter), BF16),
        vmem((count, quarter), BF16),
        vmem((count, quarter), BF16),
        vmem((count, block), BF16),
        vmem((count, block), F32),
        vmem((count, 8), F32),
        vmem((count, 8), F32),
        pltpu.SemaphoreType.DMA((10,)),
        pltpu.SemaphoreType.DMA((COPIES,)),
        pltpu.SemaphoreType.DMA((COPIES,)),
    ]
    return pl.pallas_call(
        pair_kernel,
        out_shape=pltpu.VMEM((count, quarter), BF16),
        in_specs=[pl.BlockSpec(memory_space=pltpu.HBM)] * 10,
        out_specs=pl.BlockSpec(memory_space=vmem),
        scratch_shapes=scratch,
        compiler_params=pltpu.CompilerParams(
            collective_id=0, has_side_effects=True, vmem_limit_bytes=VMEM_LIMIT
        ),
    )(
        *(
            pltpu.with_memory_space_constraint(operand, pltpu.HBM)
            for operand in (
                tokens,
                norm_gain[None, :],
                routing.T,
                route_weight.T,
                w_gate[0],
                w_up[0],
                w_down[0],
                w_branch_in,
                w_branch_out,
                branch_gate[None, :],
            )
        )
    )


def solution(mesh):
    return jax.shard_map(
        pair_body if mesh.shape["ep"] == 2 * GROUPS and mesh.shape["tp"] == 4 else body,
        mesh=mesh,
        in_specs=(
            P("ep", "tp"),
            P("tp"),
            P("ep", None),
            P("ep", None),
            P("ep", "tp", None),
            P("ep", "tp", None),
            P("ep", None, "tp"),
            P("ep", "tp"),
            P("tp", "ep"),
            P("tp"),
        ),
        out_specs=P("ep", "tp"),
        check_vma=False,
    )
```

```python
import functools

import jax
import jax.numpy as jnp
from jax import lax
from jax.experimental import pallas as pl
from jax.experimental.pallas import tpu as pltpu
from jax.sharding import PartitionSpec as P

GROUPS = 4


epsilon = 1e-06


def send_back(result):
    return lax.all_to_all(result, "ep", split_axis=0, concat_axis=0, tiled=True)


def body(
    tokens,
    norm_gain,
    routing,
    route_weight,
    w_gate,
    w_up,
    w_down,
    w_branch_in,
    w_branch_out,
    branch_gate,
):
    token_count, quarter = tokens.shape
    full_width = quarter * lax.axis_size("tp")
    floats = tokens.astype(jnp.float32)
    squares = lax.psum(jnp.sum(floats * floats, axis=1), "tp")
    normed = (floats * lax.rsqrt(squares[:, None] / full_width + epsilon) * norm_gain).astype(
        jnp.bfloat16
    )
    expert_count = lax.axis_size("ep") * w_gate.shape[0]
    capacity = token_count // (expert_count // GROUPS)
    flat_ids = routing.reshape(-1)
    one_hot = (flat_ids[:, None] == jnp.arange(expert_count, dtype=jnp.int32)[None, :]).astype(
        jnp.int32
    )
    before = jnp.cumsum(one_hot, axis=0) - one_hot
    position = flat_ids * capacity + jnp.sum(before * one_hot, axis=1)
    copies = jnp.repeat(normed, 2, axis=0)
    buffer = jnp.zeros((expert_count * capacity, quarter), jnp.bfloat16).at[position].set(copies)
    buffer = buffer.reshape(expert_count, capacity, quarter)
    gate_whole, up_whole, down_whole = (
        lax.all_gather(w_gate[0], "tp", axis=0, tiled=True),
        lax.all_gather(w_up[0], "tp", axis=0, tiled=True),
        lax.all_gather(w_down[0], "tp", axis=1, tiled=True),
    )
    row_split = lax.all_to_all(
        lax.all_to_all(buffer, "ep", split_axis=0, concat_axis=0, tiled=True),
        "tp",
        split_axis=0,
        concat_axis=2,
        tiled=True,
    )
    slot_rows = row_split.reshape(-1, row_split.shape[2])
    gate_sum = jnp.dot(slot_rows, gate_whole, preferred_element_type=jnp.float32)
    up_sum = jnp.dot(slot_rows, up_whole, preferred_element_type=jnp.float32)
    hidden = (jax.nn.silu(gate_sum) * up_sum).astype(jnp.bfloat16)
    result = jnp.dot(hidden, down_whole, preferred_element_type=jnp.float32).astype(jnp.bfloat16)
    feature_split = lax.all_to_all(
        result.reshape(row_split.shape), "tp", split_axis=2, concat_axis=0, tiled=True
    )
    returned = send_back(feature_split)
    picked = returned.reshape(expert_count * capacity, quarter)[position].reshape(
        token_count, 2, quarter
    )
    routed = jnp.sum(picked.astype(jnp.float32) * route_weight[:, :, None], axis=1)
    branch_tokens = lax.all_to_all(normed, "tp", split_axis=0, concat_axis=1, tiled=True)
    in_cols, out_rows = (
        lax.all_gather(w_branch_in, "tp", axis=1, tiled=True),
        lax.all_gather(w_branch_out, "tp", axis=0, tiled=True),
    )
    in_whole, out_whole = (
        lax.all_gather(in_cols, "ep", axis=0, tiled=True),
        lax.all_gather(out_rows, "ep", axis=1, tiled=True),
    )
    branch_hidden = jax.nn.silu(
        jnp.dot(branch_tokens, in_whole, preferred_element_type=jnp.float32)
    ).astype(jnp.bfloat16)
    branch_local = jnp.dot(branch_hidden, out_whole, preferred_element_type=jnp.float32).astype(
        jnp.bfloat16
    )
    branch = lax.all_to_all(branch_local, "tp", split_axis=1, concat_axis=0, tiled=True)
    return (routed + jax.nn.sigmoid(branch_gate) * branch.astype(jnp.float32)).astype(jnp.bfloat16)


BF16, F32 = jnp.bfloat16, jnp.float32
COPIES = 61
VMEM_LIMIT = 46 * 1024 * 1024


def dot(a, b):
    return jnp.dot(a, b, preferred_element_type=F32)


def dot_nt(a, b):
    return lax.dot_general(a, b, (((1,), (1,)), ((), ())), preferred_element_type=F32)


def silu(v):
    return v / (1.0 + jnp.exp(-v))


def pair_kernel(
    tokens_hbm,
    gain_hbm,
    routing_hbm,
    route_weight_hbm,
    w_gate,
    w_up,
    w_down,
    w_in,
    w_out,
    branch_gate_hbm,
    out,
    tokens,
    gain,
    routing,
    route_weight,
    branch_gate,
    gate_all,
    up_all,
    down_all,
    squares,
    scaled,
    branch_all,
    chosen,
    slots_out,
    slots,
    slots_s,
    scale_out,
    scale,
    scale_col,
    part_out,
    part_own,
    part_in,
    hidden,
    half_out,
    half_own,
    half_in,
    back_out,
    back,
    fold_out,
    fold_own,
    fold_in,
    cross_out,
    cross_in,
    branch_hidden,
    branch_acc,
    code_col,
    factor_col,
    load_sem,
    send_sem,
    recv_sem,
):
    ep, tp = lax.axis_index("ep"), lax.axis_index("tp")
    z, y, x, c = ep // 2, ep % 2, tp // 2, tp % 2
    token_count, quarter = tokens.shape
    ff = w_gate.shape[1]
    capacity = slots.shape[1]
    half = capacity // 2
    block = w_in.shape[0]

    def at(zz, yy, xx, cc):
        return (zz * 2 + yy, xx * 2 + cc)

    sibling = at(z, y, x, 1 - c)
    across = at(z, y, 1 - x, c)
    diagonal = at(z, y, 1 - x, 1 - c)
    pair = at(z, 1 - y, x, c)
    pair_user = at(z, 1 - y, x, y)
    pair_other = at(z, 1 - y, x, 1 - c)
    level = [z, z + 1 - 2 * (z % 2), (z + 2) % GROUPS, GROUPS - 1 - z]
    peer_of = [None] + [at(level[m], y, x, c) for m in range(1, GROUPS)]
    up = at((z + 1) % GROUPS, y, x, c)
    down = at((z + GROUPS - 1) % GROUPS, y, x, c)

    barrier = pltpu.get_barrier_semaphore()
    peers = [sibling, across, diagonal, pair, pair_other] + peer_of[1:]
    for peer in peers:
        pl.semaphore_signal(
            barrier, inc=1, device_id=peer, device_id_type=pl.DeviceIdType.MESH
        )

    loads = [
        pltpu.make_async_copy(source, target, load_sem.at[number])
        for number, (source, target) in enumerate(
            (
                (routing_hbm, routing),
                (tokens_hbm, tokens),
                (gain_hbm, gain),
                (route_weight_hbm, route_weight),
                (branch_gate_hbm, branch_gate),
                (w_in, branch_all.at[y, z, 0]),
                (w_out, branch_all.at[y, z, 1]),
            )
        )
    ]
    for load in loads:
        load.start()

    weights_of = ((w_gate, gate_all), (w_up, up_all), (w_down, down_all))

    def weight_load(k):
        source, target = weights_of[k]
        return pltpu.make_async_copy(source, target.at[c], load_sem.at[len(loads) + k])

    @pl.when(c == y)
    def _():
        for k in range(3):
            weight_load(k).start()

    loads[0].wait()
    ids = routing[0:1, :]
    group = lax.shift_right_logical(ids, 1)
    rows16 = lax.broadcasted_iota(jnp.int32, (16, token_count), 0)
    member = jnp.where(rows16 == group, 1.0, 0.0)
    earlier = jnp.where(
        lax.broadcasted_iota(jnp.int32, (token_count, token_count), 0)
        < lax.broadcasted_iota(jnp.int32, (token_count, token_count), 1),
        1.0,
        0.0,
    ).astype(BF16)
    before = dot(member.astype(BF16), earlier)
    place = jnp.sum(member * before, axis=0, keepdims=True)
    code = group.astype(F32) * capacity + place

    loads[1].wait()
    loads[2].wait()
    floats = tokens[...].astype(F32)
    scaled[0] = (floats * gain[...]).astype(BF16)
    exact = floats * floats
    high = exact.astype(BF16)
    low = (exact - high.astype(F32)).astype(BF16)
    ones = jnp.ones((16, quarter), BF16)
    squares[0] = (dot_nt(ones, high) + dot_nt(ones, low))[:1]

    slot_row = lax.broadcasted_iota(jnp.int32, (capacity, token_count), 0)

    def choose_rows(s, where, target):
        wanted = (slot_row + where * capacity).astype(F32)
        chosen[s] = jnp.where(wanted == code, 1.0, 0.0).astype(BF16)
        target[s] = dot(chosen[s], scaled[0]).astype(BF16)

    outer = (z == 0) | (z == GROUPS - 1)
    near = jnp.where(outer, 1, 2)
    choose_rows(near, jnp.where(outer, level[1], level[2]), slots_out)

    pl.semaphore_wait(barrier, len(peers))

    started = {}

    def is_own(s):
        return isinstance(s, int) and s == 0

    def key_of(number):
        return number if isinstance(number, int) else ("dynamic", len(started))

    def wait_for(number, target):
        pltpu.make_async_remote_copy(
            src_ref=target,
            dst_ref=target,
            send_sem=send_sem.at[number],
            recv_sem=recv_sem.at[number],
            device_id=sibling,
            device_id_type=pl.DeviceIdType.MESH,
        ).wait_recv()

    def send(number, source, target, device):
        copy = pltpu.make_async_remote_copy(
            src_ref=source,
            dst_ref=target,
            send_sem=send_sem.at[number],
            recv_sem=recv_sem.at[number],
            device_id=device,
            device_id_type=pl.DeviceIdType.MESH,
        )
        copy.start()
        started[key_of(number)] = copy

    def send_if(condition, number, source, target, device):
        copy = pltpu.make_async_remote_copy(
            src_ref=source,
            dst_ref=target,
            send_sem=send_sem.at[number],
            recv_sem=recv_sem.at[number],
            device_id=device,
            device_id_type=pl.DeviceIdType.MESH,
        )

        @pl.when(condition)
        def _():
            copy.start()

        started[number] = copy

    def arrived(number):
        started[number].wait_recv()

    def weight_copy(k, sem, device):
        source, target = weights_of[k]
        return pltpu.make_async_remote_copy(
            src_ref=source,
            dst_ref=target.at[c],
            send_sem=send_sem.at[2 * k + sem],
            recv_sem=recv_sem.at[2 * k + c],
            device_id=device,
            device_id_type=pl.DeviceIdType.MESH,
        )

    def send_slots(s):
        send(19 + s, slots_out.at[s], slots.at[s], peer_of[s])

    def send_slots_if(condition, s):
        send_if(condition, 19 + s, slots_out.at[s], slots.at[s], peer_of[s])

    def send_scale(s):
        send(22 + s, scale_out.at[s], scale.at[s], peer_of[s])

    def relay(hop, upward):
        number = (12 if upward else 47) + hop - 1
        held = z - (hop - 1) if upward else z + (hop - 1)
        came = z - hop if upward else z + hop
        held, came = (held + GROUPS) % GROUPS, (came + GROUPS) % GROUPS
        sends = (z <= GROUPS - 2) & (z >= hop - 1)
        gets = z >= hop
        if not upward:
            sends = (z >= 1) & (z <= GROUPS - hop)
            gets = z <= GROUPS - 1 - hop

        def copy(row):
            return pltpu.make_async_remote_copy(
                src_ref=branch_all.at[y, row],
                dst_ref=branch_all.at[y, row],
                send_sem=send_sem.at[number],
                recv_sem=recv_sem.at[number],
                device_id=up if upward else down,
                device_id_type=pl.DeviceIdType.MESH,
            )

        return sends, gets, lambda: copy(held), lambda: copy(came)

    def relay_start(hop):
        for upward in (True, False):
            sends, _, outgoing, _ = relay(hop, upward)

            @pl.when(sends)
            def _():
                outgoing().start()

    def relay_arrived(hop):
        for upward in (True, False):
            _, gets, _, incoming = relay(hop, upward)

            @pl.when(gets)
            def _():
                incoming().wait_recv()

    def relay_sent(hop):
        for upward in (True, False):
            sends, _, outgoing, _ = relay(hop, upward)

            @pl.when(sends)
            def _():
                outgoing().wait_send()

    send(7, squares.at[0], squares.at[2], across)
    send(8, squares.at[0], squares.at[3], diagonal)
    send(6, squares.at[0], squares.at[1], sibling)
    early = c == y
    send_slots_if(outer, 1)
    send_slots_if(~outer, 2)
    part_rows = token_count // 2
    first_rows, last_rows = pl.ds(0, part_rows), pl.ds(part_rows, part_rows)

    def send_tokens(number, rows):
        return number, scaled.at[0, rows], scaled.at[2, rows], across

    send(*send_tokens(10, first_rows))
    send_if(~early, *send_tokens(57, last_rows))
    for k in range(3):
        weight_copy(k, 0, pair_user).start()

    @pl.when(c != y)
    def _():
        for k in range(3):
            weight_copy(k, 1, sibling).start()

    choose_rows(3 - near, jnp.where(outer, level[2], level[1]), slots_out)
    send_slots_if(outer, 2)
    loads[5].wait()
    loads[6].wait()
    relay_start(1)
    send(9, scaled.at[0], scaled.at[1], sibling)

    def weight_arrived(k):
        source, target = weights_of[k]

        def wait(h):
            pltpu.make_async_remote_copy(
                src_ref=source,
                dst_ref=target.at[h],
                send_sem=send_sem.at[2 * k],
                recv_sem=recv_sem.at[2 * k + h],
                device_id=sibling,
                device_id_type=pl.DeviceIdType.MESH,
            ).wait_recv()

        wait(1 - c)

        @pl.when(c != y)
        def _():
            wait(c)

        @pl.when(c == y)
        def _():
            weight_load(k).wait()

    def pair_send(m):
        rows = branch_all.at[y, level[m]]
        send(15 + m, rows, rows, pair)

    choose_rows(0, level[0], slots)
    send(26, slots.at[0], slots_s.at[0], sibling)
    choose_rows(3, level[3], slots_out)
    pair_send(0)

    loads[3].wait()
    loads[4].wait()
    first, second = route_weight[0:1, :], route_weight[1:2, :]
    even_first = (ids & 1) == 0
    for_even = jnp.where(even_first, first, second)
    for_odd = jnp.where(even_first, second, first)
    for number in (6, 7, 8):
        arrived(number)
    total = squares[0] + squares[1] + squares[2] + squares[3]
    factor = lax.rsqrt(total / (4 * quarter) + epsilon)
    factor_col[...] = jnp.transpose(jnp.broadcast_to(factor, (8, token_count)))
    code_col[...] = jnp.transpose(jnp.broadcast_to(code, (8, token_count)))
    weights = jnp.where(
        rows16 == 0, for_even, jnp.where(rows16 == 1, for_odd, factor)
    )
    weights_high = weights.astype(BF16)
    weights_low = (weights - weights_high.astype(F32)).astype(BF16)
    for s in (2, 3, 1, 0):
        slot_weights = (dot_nt(weights_high, chosen[s]) + dot_nt(weights_low, chosen[s]))[:4]
        if s == 0:
            scale[0] = slot_weights
        else:
            scale_out[s] = slot_weights
            send_scale(s)
    send_slots_if(outer, 3)

    def project(s, start, weights):
        own = slots[s, pl.ds(start, half), :]
        other = slots_s[s, pl.ds(start, half), :]
        return dot(own, weights[c]) + dot(other, weights[1 - c])

    mine = pl.multiple_of(x * half, half)
    theirs = pl.multiple_of((1 - x) * half, half)

    def forward(s):
        wait_for(19 + s, slots.at[s])
        send(26 + s, slots.at[s], slots_s.at[s], sibling)

    sides = (slice(0, ff), slice(ff, 2 * ff))

    def stage_a(s):
        wait_for(26 + s, slots_s.at[s])
        for side, weights in zip(sides, (gate_all, up_all)):
            part_out[s, :, side] = project(s, theirs, weights).astype(BF16)
        send(30 + s, part_out.at[s], part_in.at[s], across)
        for side, weights in zip(sides, (gate_all, up_all)):
            part_own[s, :, side] = project(s, mine, weights)

    def stage_a_up_if(condition):
        number, side = 50, sides[1]
        copy = pltpu.make_async_remote_copy(
            src_ref=part_out.at[0, :, side],
            dst_ref=part_in.at[0, :, side],
            send_sem=send_sem.at[number],
            recv_sem=recv_sem.at[number],
            device_id=across,
            device_id_type=pl.DeviceIdType.MESH,
        )
        started[number] = copy

        @pl.when(condition)
        def _():
            part_out[0, :, side] = project(0, theirs, up_all).astype(BF16)
            copy.start()
            part_own[0, :, side] = project(0, mine, up_all)

    def stage_a_side(s, k):
        if k == 0:
            wait_for(26 + s, slots_s.at[s])
        side, weights = sides[k], (gate_all, up_all)[k]
        part_out[s, :, side] = project(s, theirs, weights).astype(BF16)
        number = 30 + s if k == 0 else 50 + s
        send(number, part_out.at[s, :, side], part_in.at[s, :, side], across)
        part_own[s, :, side] = project(s, mine, weights)

    def stage_b(s, sided=False):
        if not is_own(s):
            wait_for(22 + s, scale.at[s])
        scale_col[s] = jnp.transpose(jnp.concatenate([scale[s], scale[s]], axis=0))
        if is_own(s) or sided:
            wait_for(30 + s, part_in.at[s, :, sides[0]])
            wait_for(50 + s, part_in.at[s, :, sides[1]])
        else:
            wait_for(30 + s, part_in.at[s])
        rescale = scale_col[s, pl.ds(mine, half), 2:3]
        gate_sum = (part_own[s, :, :ff] + part_in[s, :, :ff].astype(F32)) * rescale
        up_sum = (part_own[s, :, ff:] + part_in[s, :, ff:].astype(F32)) * rescale
        hidden[s, pl.ds(mine, half), :] = (silu(gate_sum) * up_sum).astype(BF16)
        kept = hidden.at[s, pl.ds(mine, half), :]
        send(34 + s, kept, kept, across)

    def stage_c(s):
        wait_for(34 + s, hidden.at[s, pl.ds(theirs, half), :])
        weight = jnp.where(c == 0, scale_col[s, :, 0:1], scale_col[s, :, 1:2])
        units = hidden[s]
        half_out[s] = (dot(units, down_all[1 - c]) * weight).astype(BF16)
        send(38 + s, half_out.at[s], half_in.at[s], sibling)
        half_own[s] = dot(units, down_all[c]) * weight

    def stage_d(s):
        wait_for(38 + s, half_in.at[s])
        both = (half_own[s] + half_in[s].astype(F32)).astype(BF16)
        if is_own(s):
            back[0] = both
        else:
            back_out[s] = both
            zone = level[s] if isinstance(s, int) else jnp.where(s == 1, level[1], level[3])
            send(41 + s, back_out.at[s], back.at[s], at(zone, y, x, c))

    quarters = (tp, x * 2 + 1 - c, (1 - x) * 2 + c, (1 - x) * 2 + 1 - c)

    def branch_sum(members, first=False, last=False):
        sums = jnp.zeros((token_count, block), F32) if first else branch_acc[...]
        for m in members:
            wait_for(15 + m, branch_all.at[1 - y, level[m]])
            q = level[m]
            k = (x + q // 2) % 2 * 2 + (c + q) % 2
            sums = sums + dot(scaled[k, :, :block], branch_all[0, q, 0])
            sums = sums + dot(scaled[k, :, block:], branch_all[1, q, 0])
        if last:
            branch_hidden[...] = silu(sums * factor_col[:, 0:1]).astype(BF16)
        else:
            branch_acc[...] = sums

    def branch_part(q, side):
        return dot(branch_hidden[...], branch_all[side, q, 1])

    left, right = slice(0, block), slice(block, 2 * block)

    def branch_fold():
        for number, side, columns in ((54, 0, left), (55, 1, right)):
            fold_out[1, :, columns] = branch_part(quarters[3], side).astype(BF16)
            send(number, fold_out.at[1, :, columns], fold_in.at[1, :, columns], sibling)

    def branch_fold_own():
        for side, columns in ((0, left), (1, right)):
            fold_out[0, :, columns] = branch_part(quarters[1], side).astype(BF16)
        send(58, fold_out.at[0], fold_in.at[0], sibling)

    def branch_cross(number, side, rows):
        columns = (left, right)[side]
        cross_out[rows, columns] = (
            dot(branch_hidden[rows], branch_all[side, quarters[2], 1])
            + fold_in[1, rows, columns].astype(F32)
        ).astype(BF16)
        send(number, cross_out.at[rows, columns], cross_in.at[rows, columns], across)

    def branch_own():
        arrived(58)
        for side in range(2):
            columns = slice(side * block, (side + 1) * block)
            fold_own[:, columns] = branch_part(quarters[0], side) + fold_in[
                0, :, columns
            ].astype(F32)

    slot_lane = lax.broadcasted_iota(jnp.int32, (token_count, capacity), 1)

    def restore(s):
        if s:
            wait_for(41 + s, back.at[s])
        wanted = (slot_lane + level[s] * capacity).astype(F32)
        choose = jnp.where(wanted == code_col[:, 0:1], 1.0, 0.0).astype(BF16)
        return dot(choose, back[s])

    first = jnp.where(outer, 3, 1)
    last = 4 - first
    weight_arrived(0)
    stage_a_side(0, 0)

    @pl.when(early)
    def _():
        weight_arrived(1)

    stage_a_up_if(early)
    send_if(early & ~outer, *send_tokens(57, last_rows))
    forward(2)
    send_slots_if(~outer, 1)
    stage_a_side(2, 0)

    @pl.when(~early)
    def _():
        weight_arrived(1)

    stage_a_side(2, 1)
    send_if(early & outer, *send_tokens(57, last_rows))
    stage_a_up_if(~early)
    relay_arrived(1)
    relay_start(2)
    send_slots_if(~outer, 3)
    pair_send(1)
    stage_b(2, True)
    stage_b(0)
    forward(first)
    stage_a_side(first, 0)
    stage_a_side(first, 1)
    weight_arrived(2)
    stage_c(2)
    relay_arrived(2)
    relay_start(3)
    pair_send(2)
    stage_c(0)
    stage_d(0)
    arrived(10)
    arrived(57)
    send(11, scaled.at[2], scaled.at[3], sibling)
    forward(last)
    stage_d(2)
    stage_a_side(last, 0)
    relay_arrived(3)
    pair_send(3)
    stage_b(first, True)
    stage_a_side(last, 1)
    arrived(9)
    arrived(11)
    branch_sum((0, 1, 2), first=True)
    branch_sum((3,), last=True)
    branch_fold()
    arrived(54)
    branch_cross(46, 0, slice(0, capacity))
    stage_c(first)
    stage_d(first)
    stage_b(last, True)
    branch_cross(59, 0, slice(capacity, token_count))
    arrived(55)
    branch_cross(60, 1, slice(0, token_count))
    branch_fold_own()
    stage_c(last)
    stage_d(last)
    branch_own()

    half_own_sum = restore(0)
    half_own_sum = half_own_sum + restore(2)
    half_own_sum = half_own_sum + restore(3)
    half_own_sum = half_own_sum + restore(1)
    arrived(46)
    arrived(59)
    arrived(60)
    branch = fold_own[...] + cross_in[...].astype(F32)
    gate = 1.0 / (1.0 + jnp.exp(-branch_gate[...]))
    out[...] = (half_own_sum + gate * branch).astype(BF16)
    for copy in started.values():
        copy.wait_send()
    for hop in range(1, GROUPS):
        relay_sent(hop)
    for k in range(3):
        weight_copy(k, 0, pair_user).wait_send()

    @pl.when(c != y)
    def _():
        for k in range(3):
            weight_copy(k, 1, sibling).wait_send()


def pair_body(
    tokens,
    norm_gain,
    routing,
    route_weight,
    w_gate,
    w_up,
    w_down,
    w_branch_in,
    w_branch_out,
    branch_gate,
):
    count, quarter = tokens.shape
    ff = w_gate.shape[2]
    block = w_branch_in.shape[0]
    cap = count // 2
    half = cap // 2
    vmem = pltpu.VMEM
    rows = (GROUPS, cap, quarter)
    scratch = [
        vmem((count, quarter), BF16),
        vmem((1, quarter), F32),
        vmem((2, count), jnp.int32),
        vmem((2, count), F32),
        vmem((1, quarter), F32),
        vmem((2, quarter, ff), BF16),
        vmem((2, quarter, ff), BF16),
        vmem((2, ff, quarter), BF16),
        vmem((4, 1, count), F32),
        vmem((4, count, quarter), BF16),
        vmem((2, GROUPS, 2, block, block), BF16),
        vmem((GROUPS, cap, count), BF16),
        vmem(rows, BF16),
        vmem(rows, BF16),
        vmem(rows, BF16),
        vmem((GROUPS, 4, cap), F32),
        vmem((GROUPS, 4, cap), F32),
        vmem((GROUPS, cap, 8), F32),
        vmem((GROUPS, half, 2 * ff), BF16),
        vmem((GROUPS, half, 2 * ff), F32),
        vmem((GROUPS, half, 2 * ff), BF16),
        vmem((GROUPS, cap, ff), BF16),
        vmem(rows, BF16),
        vmem(rows, F32),
        vmem(rows, BF16),
        vmem(rows, BF16),
        vmem(rows, BF16),
        vmem((2, count, quarter), BF16),
        vmem((count, quarter), F32),
        vmem((2, count, quarter), BF16),
        vmem((count, quarter), BF16),
        vmem((count, quarter), BF16),
        vmem((count, block), BF16),
        vmem((count, block), F32),
        vmem((count, 8), F32),
        vmem((count, 8), F32),
        pltpu.SemaphoreType.DMA((10,)),
        pltpu.SemaphoreType.DMA((COPIES,)),
        pltpu.SemaphoreType.DMA((COPIES,)),
    ]
    return pl.pallas_call(
        pair_kernel,
        out_shape=pltpu.VMEM((count, quarter), BF16),
        in_specs=[pl.BlockSpec(memory_space=pltpu.HBM)] * 10,
        out_specs=pl.BlockSpec(memory_space=vmem),
        scratch_shapes=scratch,
        compiler_params=pltpu.CompilerParams(
            collective_id=0, has_side_effects=True, vmem_limit_bytes=VMEM_LIMIT
        ),
    )(
        *(
            pltpu.with_memory_space_constraint(operand, pltpu.HBM)
            for operand in (
                tokens,
                norm_gain[None, :],
                routing.T,
                route_weight.T,
                w_gate[0],
                w_up[0],
                w_down[0],
                w_branch_in,
                w_branch_out,
                branch_gate[None, :],
            )
        )
    )


def solution(mesh):
    return jax.shard_map(
        pair_body if mesh.shape["ep"] == 2 * GROUPS and mesh.shape["tp"] == 4 else body,
        mesh=mesh,
        in_specs=(
            P("ep", "tp"),
            P("tp"),
            P("ep", None),
            P("ep", None),
            P("ep", "tp", None),
            P("ep", "tp", None),
            P("ep", None, "tp"),
            P("ep", "tp"),
            P("tp", "ep"),
            P("tp"),
        ),
        out_specs=P("ep", "tp"),
        check_vma=False,
    )
```

```python
import functools

import jax
import jax.numpy as jnp
from jax import lax
from jax.experimental import pallas as pl
from jax.experimental.pallas import tpu as pltpu
from jax.sharding import PartitionSpec as P

GROUPS = 4


epsilon = 1e-06


def send_back(result):
    return lax.all_to_all(result, "ep", split_axis=0, concat_axis=0, tiled=True)


def body(
    tokens,
    norm_gain,
    routing,
    route_weight,
    w_gate,
    w_up,
    w_down,
    w_branch_in,
    w_branch_out,
    branch_gate,
):
    token_count, quarter = tokens.shape
    full_width = quarter * lax.axis_size("tp")
    floats = tokens.astype(jnp.float32)
    squares = lax.psum(jnp.sum(floats * floats, axis=1), "tp")
    normed = (floats * lax.rsqrt(squares[:, None] / full_width + epsilon) * norm_gain).astype(
        jnp.bfloat16
    )
    expert_count = lax.axis_size("ep") * w_gate.shape[0]
    capacity = token_count // (expert_count // GROUPS)
    flat_ids = routing.reshape(-1)
    one_hot = (flat_ids[:, None] == jnp.arange(expert_count, dtype=jnp.int32)[None, :]).astype(
        jnp.int32
    )
    before = jnp.cumsum(one_hot, axis=0) - one_hot
    position = flat_ids * capacity + jnp.sum(before * one_hot, axis=1)
    copies = jnp.repeat(normed, 2, axis=0)
    buffer = jnp.zeros((expert_count * capacity, quarter), jnp.bfloat16).at[position].set(copies)
    buffer = buffer.reshape(expert_count, capacity, quarter)
    gate_whole, up_whole, down_whole = (
        lax.all_gather(w_gate[0], "tp", axis=0, tiled=True),
        lax.all_gather(w_up[0], "tp", axis=0, tiled=True),
        lax.all_gather(w_down[0], "tp", axis=1, tiled=True),
    )
    row_split = lax.all_to_all(
        lax.all_to_all(buffer, "ep", split_axis=0, concat_axis=0, tiled=True),
        "tp",
        split_axis=0,
        concat_axis=2,
        tiled=True,
    )
    slot_rows = row_split.reshape(-1, row_split.shape[2])
    gate_sum = jnp.dot(slot_rows, gate_whole, preferred_element_type=jnp.float32)
    up_sum = jnp.dot(slot_rows, up_whole, preferred_element_type=jnp.float32)
    hidden = (jax.nn.silu(gate_sum) * up_sum).astype(jnp.bfloat16)
    result = jnp.dot(hidden, down_whole, preferred_element_type=jnp.float32).astype(jnp.bfloat16)
    feature_split = lax.all_to_all(
        result.reshape(row_split.shape), "tp", split_axis=2, concat_axis=0, tiled=True
    )
    returned = send_back(feature_split)
    picked = returned.reshape(expert_count * capacity, quarter)[position].reshape(
        token_count, 2, quarter
    )
    routed = jnp.sum(picked.astype(jnp.float32) * route_weight[:, :, None], axis=1)
    branch_tokens = lax.all_to_all(normed, "tp", split_axis=0, concat_axis=1, tiled=True)
    in_cols, out_rows = (
        lax.all_gather(w_branch_in, "tp", axis=1, tiled=True),
        lax.all_gather(w_branch_out, "tp", axis=0, tiled=True),
    )
    in_whole, out_whole = (
        lax.all_gather(in_cols, "ep", axis=0, tiled=True),
        lax.all_gather(out_rows, "ep", axis=1, tiled=True),
    )
    branch_hidden = jax.nn.silu(
        jnp.dot(branch_tokens, in_whole, preferred_element_type=jnp.float32)
    ).astype(jnp.bfloat16)
    branch_local = jnp.dot(branch_hidden, out_whole, preferred_element_type=jnp.float32).astype(
        jnp.bfloat16
    )
    branch = lax.all_to_all(branch_local, "tp", split_axis=1, concat_axis=0, tiled=True)
    return (routed + jax.nn.sigmoid(branch_gate) * branch.astype(jnp.float32)).astype(jnp.bfloat16)


BF16, F32 = jnp.bfloat16, jnp.float32
COPIES = 61
VMEM_LIMIT = 46 * 1024 * 1024


def dot(a, b):
    return jnp.dot(a, b, preferred_element_type=F32)


def dot_nt(a, b):
    return lax.dot_general(a, b, (((1,), (1,)), ((), ())), preferred_element_type=F32)


def silu(v):
    return v / (1.0 + jnp.exp(-v))


def pair_kernel(
    tokens_hbm,
    gain_hbm,
    routing_hbm,
    route_weight_hbm,
    w_gate,
    w_up,
    w_down,
    w_in,
    w_out,
    branch_gate_hbm,
    out,
    tokens,
    gain,
    routing,
    route_weight,
    branch_gate,
    gate_all,
    up_all,
    down_all,
    squares,
    scaled,
    branch_all,
    chosen,
    slots_out,
    slots,
    slots_s,
    scale_out,
    scale,
    scale_col,
    part_out,
    part_own,
    part_in,
    hidden,
    half_out,
    half_own,
    half_in,
    back_out,
    back,
    fold_out,
    fold_own,
    fold_in,
    cross_out,
    cross_in,
    branch_hidden,
    branch_acc,
    code_col,
    factor_col,
    load_sem,
    send_sem,
    recv_sem,
):
    ep, tp = lax.axis_index("ep"), lax.axis_index("tp")
    z, y, x, c = ep // 2, ep % 2, tp // 2, tp % 2
    token_count, quarter = tokens.shape
    ff = w_gate.shape[1]
    capacity = slots.shape[1]
    half = capacity // 2
    block = w_in.shape[0]

    def at(zz, yy, xx, cc):
        return (zz * 2 + yy, xx * 2 + cc)

    sibling = at(z, y, x, 1 - c)
    across = at(z, y, 1 - x, c)
    diagonal = at(z, y, 1 - x, 1 - c)
    pair = at(z, 1 - y, x, c)
    pair_user = at(z, 1 - y, x, y)
    pair_other = at(z, 1 - y, x, 1 - c)
    level = [z, z + 1 - 2 * (z % 2), (z + 2) % GROUPS, GROUPS - 1 - z]
    peer_of = [None] + [at(level[m], y, x, c) for m in range(1, GROUPS)]
    up = at((z + 1) % GROUPS, y, x, c)
    down = at((z + GROUPS - 1) % GROUPS, y, x, c)

    barrier = pltpu.get_barrier_semaphore()
    peers = [sibling, across, diagonal, pair, pair_other] + peer_of[1:]
    for peer in peers:
        pl.semaphore_signal(
            barrier, inc=1, device_id=peer, device_id_type=pl.DeviceIdType.MESH
        )

    loads = [
        pltpu.make_async_copy(source, target, load_sem.at[number])
        for number, (source, target) in enumerate(
            (
                (routing_hbm, routing),
                (tokens_hbm, tokens),
                (gain_hbm, gain),
                (route_weight_hbm, route_weight),
                (branch_gate_hbm, branch_gate),
                (w_in, branch_all.at[y, z, 0]),
                (w_out, branch_all.at[y, z, 1]),
            )
        )
    ]
    for load in loads:
        load.start()

    weights_of = ((w_gate, gate_all), (w_up, up_all), (w_down, down_all))

    def weight_load(k):
        source, target = weights_of[k]
        return pltpu.make_async_copy(source, target.at[c], load_sem.at[len(loads) + k])

    @pl.when(c == y)
    def _():
        for k in range(3):
            weight_load(k).start()

    loads[0].wait()
    ids = routing[0:1, :]
    group = lax.shift_right_logical(ids, 1)
    rows16 = lax.broadcasted_iota(jnp.int32, (16, token_count), 0)
    member = jnp.where(rows16 == group, 1.0, 0.0)
    earlier = jnp.where(
        lax.broadcasted_iota(jnp.int32, (token_count, token_count), 0)
        < lax.broadcasted_iota(jnp.int32, (token_count, token_count), 1),
        1.0,
        0.0,
    ).astype(BF16)
    before = dot(member.astype(BF16), earlier)
    place = jnp.sum(member * before, axis=0, keepdims=True)
    code = group.astype(F32) * capacity + place

    loads[1].wait()
    loads[2].wait()
    floats = tokens[...].astype(F32)
    scaled[0] = (floats * gain[...]).astype(BF16)
    exact = floats * floats
    high = exact.astype(BF16)
    low = (exact - high.astype(F32)).astype(BF16)
    ones = jnp.ones((16, quarter), BF16)
    squares[0] = (dot_nt(ones, high) + dot_nt(ones, low))[:1]

    slot_row = lax.broadcasted_iota(jnp.int32, (capacity, token_count), 0)

    def choose_rows(s, where, target):
        wanted = (slot_row + where * capacity).astype(F32)
        chosen[s] = jnp.where(wanted == code, 1.0, 0.0).astype(BF16)
        target[s] = dot(chosen[s], scaled[0]).astype(BF16)

    outer = (z == 0) | (z == GROUPS - 1)
    near = jnp.where(outer, 1, 2)
    choose_rows(near, jnp.where(outer, level[1], level[2]), slots_out)

    pl.semaphore_wait(barrier, len(peers))

    started = {}

    def is_own(s):
        return isinstance(s, int) and s == 0

    def key_of(number):
        return number if isinstance(number, int) else ("dynamic", len(started))

    def wait_for(number, target):
        pltpu.make_async_remote_copy(
            src_ref=target,
            dst_ref=target,
            send_sem=send_sem.at[number],
            recv_sem=recv_sem.at[number],
            device_id=sibling,
            device_id_type=pl.DeviceIdType.MESH,
        ).wait_recv()

    def send(number, source, target, device):
        copy = pltpu.make_async_remote_copy(
            src_ref=source,
            dst_ref=target,
            send_sem=send_sem.at[number],
            recv_sem=recv_sem.at[number],
            device_id=device,
            device_id_type=pl.DeviceIdType.MESH,
        )
        copy.start()
        started[key_of(number)] = copy

    def send_if(condition, number, source, target, device):
        copy = pltpu.make_async_remote_copy(
            src_ref=source,
            dst_ref=target,
            send_sem=send_sem.at[number],
            recv_sem=recv_sem.at[number],
            device_id=device,
            device_id_type=pl.DeviceIdType.MESH,
        )

        @pl.when(condition)
        def _():
            copy.start()

        started[number] = copy

    def arrived(number):
        started[number].wait_recv()

    def weight_copy(k, sem, device):
        source, target = weights_of[k]
        return pltpu.make_async_remote_copy(
            src_ref=source,
            dst_ref=target.at[c],
            send_sem=send_sem.at[2 * k + sem],
            recv_sem=recv_sem.at[2 * k + c],
            device_id=device,
            device_id_type=pl.DeviceIdType.MESH,
        )

    def send_slots(s):
        send(19 + s, slots_out.at[s], slots.at[s], peer_of[s])

    def send_slots_if(condition, s):
        send_if(condition, 19 + s, slots_out.at[s], slots.at[s], peer_of[s])

    def send_scale(s):
        send(22 + s, scale_out.at[s], scale.at[s], peer_of[s])

    def relay(hop, upward):
        number = (12 if upward else 47) + hop - 1
        held = z - (hop - 1) if upward else z + (hop - 1)
        came = z - hop if upward else z + hop
        held, came = (held + GROUPS) % GROUPS, (came + GROUPS) % GROUPS
        sends = (z <= GROUPS - 2) & (z >= hop - 1)
        gets = z >= hop
        if not upward:
            sends = (z >= 1) & (z <= GROUPS - hop)
            gets = z <= GROUPS - 1 - hop

        def copy(row):
            return pltpu.make_async_remote_copy(
                src_ref=branch_all.at[y, row],
                dst_ref=branch_all.at[y, row],
                send_sem=send_sem.at[number],
                recv_sem=recv_sem.at[number],
                device_id=up if upward else down,
                device_id_type=pl.DeviceIdType.MESH,
            )

        return sends, gets, lambda: copy(held), lambda: copy(came)

    def relay_start(hop):
        for upward in (True, False):
            sends, _, outgoing, _ = relay(hop, upward)

            @pl.when(sends)
            def _():
                outgoing().start()

    def relay_arrived(hop):
        for upward in (True, False):
            _, gets, _, incoming = relay(hop, upward)

            @pl.when(gets)
            def _():
                incoming().wait_recv()

    def relay_sent(hop):
        for upward in (True, False):
            sends, _, outgoing, _ = relay(hop, upward)

            @pl.when(sends)
            def _():
                outgoing().wait_send()

    send(7, squares.at[0], squares.at[2], across)
    send(8, squares.at[0], squares.at[3], diagonal)
    send(6, squares.at[0], squares.at[1], sibling)
    early = c == y
    send_slots_if(outer, 1)
    send_slots_if(~outer, 2)
    part_rows = token_count // 2
    first_rows, last_rows = pl.ds(0, part_rows), pl.ds(part_rows, part_rows)

    def send_tokens(number, rows):
        return number, scaled.at[0, rows], scaled.at[2, rows], across

    send(*send_tokens(10, first_rows))
    send_if(~early, *send_tokens(57, last_rows))
    for k in range(3):
        weight_copy(k, 0, pair_user).start()

    @pl.when(c != y)
    def _():
        for k in range(3):
            weight_copy(k, 1, sibling).start()

    choose_rows(3 - near, jnp.where(outer, level[2], level[1]), slots_out)
    send_slots_if(outer, 2)
    loads[5].wait()
    loads[6].wait()
    relay_start(1)
    send(9, scaled.at[0], scaled.at[1], sibling)

    def weight_arrived(k):
        source, target = weights_of[k]

        def wait(h):
            pltpu.make_async_remote_copy(
                src_ref=source,
                dst_ref=target.at[h],
                send_sem=send_sem.at[2 * k],
                recv_sem=recv_sem.at[2 * k + h],
                device_id=sibling,
                device_id_type=pl.DeviceIdType.MESH,
            ).wait_recv()

        wait(1 - c)

        @pl.when(c != y)
        def _():
            wait(c)

        @pl.when(c == y)
        def _():
            weight_load(k).wait()

    def pair_send(m):
        rows = branch_all.at[y, level[m]]
        send(15 + m, rows, rows, pair)

    choose_rows(0, level[0], slots)
    send(26, slots.at[0], slots_s.at[0], sibling)
    choose_rows(3, level[3], slots_out)
    pair_send(0)

    loads[3].wait()
    loads[4].wait()
    first, second = route_weight[0:1, :], route_weight[1:2, :]
    even_first = (ids & 1) == 0
    for_even = jnp.where(even_first, first, second)
    for_odd = jnp.where(even_first, second, first)
    for number in (6, 7, 8):
        arrived(number)
    total = squares[0] + squares[1] + squares[2] + squares[3]
    factor = lax.rsqrt(total / (4 * quarter) + epsilon)
    factor_col[...] = jnp.transpose(jnp.broadcast_to(factor, (8, token_count)))
    code_col[...] = jnp.transpose(jnp.broadcast_to(code, (8, token_count)))
    weights = jnp.where(
        rows16 == 0, for_even, jnp.where(rows16 == 1, for_odd, factor)
    )
    weights_high = weights.astype(BF16)
    weights_low = (weights - weights_high.astype(F32)).astype(BF16)
    for s in (2, 3, 1, 0):
        slot_weights = (dot_nt(weights_high, chosen[s]) + dot_nt(weights_low, chosen[s]))[:4]
        if s == 0:
            scale[0] = slot_weights
        else:
            scale_out[s] = slot_weights
            send_scale(s)
    send_slots_if(outer, 3)

    def project(s, start, weights):
        own = slots[s, pl.ds(start, half), :]
        other = slots_s[s, pl.ds(start, half), :]
        return dot(own, weights[c]) + dot(other, weights[1 - c])

    mine = pl.multiple_of(x * half, half)
    theirs = pl.multiple_of((1 - x) * half, half)

    def forward(s):
        wait_for(19 + s, slots.at[s])
        send(26 + s, slots.at[s], slots_s.at[s], sibling)

    sides = (slice(0, ff), slice(ff, 2 * ff))

    def stage_a(s):
        wait_for(26 + s, slots_s.at[s])
        for side, weights in zip(sides, (gate_all, up_all)):
            part_out[s, :, side] = project(s, theirs, weights).astype(BF16)
        send(30 + s, part_out.at[s], part_in.at[s], across)
        for side, weights in zip(sides, (gate_all, up_all)):
            part_own[s, :, side] = project(s, mine, weights)

    def stage_a_up_if(condition):
        number, side = 50, sides[1]
        copy = pltpu.make_async_remote_copy(
            src_ref=part_out.at[0, :, side],
            dst_ref=part_in.at[0, :, side],
            send_sem=send_sem.at[number],
            recv_sem=recv_sem.at[number],
            device_id=across,
            device_id_type=pl.DeviceIdType.MESH,
        )
        started[number] = copy

        @pl.when(condition)
        def _():
            part_out[0, :, side] = project(0, theirs, up_all).astype(BF16)
            copy.start()
            part_own[0, :, side] = project(0, mine, up_all)

    def stage_a_side(s, k):
        if k == 0:
            wait_for(26 + s, slots_s.at[s])
        side, weights = sides[k], (gate_all, up_all)[k]
        part_out[s, :, side] = project(s, theirs, weights).astype(BF16)
        number = 30 + s if k == 0 else 50 + s
        send(number, part_out.at[s, :, side], part_in.at[s, :, side], across)
        part_own[s, :, side] = project(s, mine, weights)

    def stage_b(s, sided=False):
        if not is_own(s):
            wait_for(22 + s, scale.at[s])
        scale_col[s] = jnp.transpose(jnp.concatenate([scale[s], scale[s]], axis=0))
        if is_own(s) or sided:
            wait_for(30 + s, part_in.at[s, :, sides[0]])
            wait_for(50 + s, part_in.at[s, :, sides[1]])
        else:
            wait_for(30 + s, part_in.at[s])
        rescale = scale_col[s, pl.ds(mine, half), 2:3]
        gate_sum = (part_own[s, :, :ff] + part_in[s, :, :ff].astype(F32)) * rescale
        up_sum = (part_own[s, :, ff:] + part_in[s, :, ff:].astype(F32)) * rescale
        hidden[s, pl.ds(mine, half), :] = (silu(gate_sum) * up_sum).astype(BF16)
        kept = hidden.at[s, pl.ds(mine, half), :]
        send(34 + s, kept, kept, across)

    def stage_c(s):
        wait_for(34 + s, hidden.at[s, pl.ds(theirs, half), :])
        weight = jnp.where(c == 0, scale_col[s, :, 0:1], scale_col[s, :, 1:2])
        units = hidden[s]
        half_out[s] = (dot(units, down_all[1 - c]) * weight).astype(BF16)
        send(38 + s, half_out.at[s], half_in.at[s], sibling)
        half_own[s] = dot(units, down_all[c]) * weight

    def stage_d(s):
        wait_for(38 + s, half_in.at[s])
        both = (half_own[s] + half_in[s].astype(F32)).astype(BF16)
        if is_own(s):
            back[0] = both
        else:
            back_out[s] = both
            zone = level[s] if isinstance(s, int) else jnp.where(s == 1, level[1], level[3])
            send(41 + s, back_out.at[s], back.at[s], at(zone, y, x, c))

    quarters = (tp, x * 2 + 1 - c, (1 - x) * 2 + c, (1 - x) * 2 + 1 - c)

    def branch_sum(members, first=False, last=False):
        sums = jnp.zeros((token_count, block), F32) if first else branch_acc[...]
        for m in members:
            wait_for(15 + m, branch_all.at[1 - y, level[m]])
            q = level[m]
            k = (x + q // 2) % 2 * 2 + (c + q) % 2
            sums = sums + dot(scaled[k, :, :block], branch_all[0, q, 0])
            sums = sums + dot(scaled[k, :, block:], branch_all[1, q, 0])
        if last:
            branch_hidden[...] = silu(sums * factor_col[:, 0:1]).astype(BF16)
        else:
            branch_acc[...] = sums

    def branch_part(q, side):
        return dot(branch_hidden[...], branch_all[side, q, 1])

    left, right = slice(0, block), slice(block, 2 * block)

    def branch_fold():
        for number, side, columns in ((54, 0, left), (55, 1, right)):
            fold_out[1, :, columns] = branch_part(quarters[3], side).astype(BF16)
            send(number, fold_out.at[1, :, columns], fold_in.at[1, :, columns], sibling)

    def branch_fold_own():
        for side, columns in ((0, left), (1, right)):
            fold_out[0, :, columns] = branch_part(quarters[1], side).astype(BF16)
        send(58, fold_out.at[0], fold_in.at[0], sibling)

    def branch_cross(side, rows):
        columns = (left, right)[side]
        cross_out[rows, columns] = (
            dot(branch_hidden[rows], branch_all[side, quarters[2], 1])
            + fold_in[1, rows, columns].astype(F32)
        ).astype(BF16)

    def cross_piece(number, side, rows):
        columns = (left, right)[side]
        return number, cross_out.at[rows, columns], cross_in.at[rows, columns], across

    def branch_own():
        arrived(58)
        for side in range(2):
            columns = slice(side * block, (side + 1) * block)
            fold_own[:, columns] = branch_part(quarters[0], side) + fold_in[
                0, :, columns
            ].astype(F32)

    slot_lane = lax.broadcasted_iota(jnp.int32, (token_count, capacity), 1)

    def restore(s):
        if s:
            wait_for(41 + s, back.at[s])
        wanted = (slot_lane + level[s] * capacity).astype(F32)
        choose = jnp.where(wanted == code_col[:, 0:1], 1.0, 0.0).astype(BF16)
        return dot(choose, back[s])

    first = jnp.where(outer, 3, 1)
    last = 4 - first
    weight_arrived(0)
    stage_a_side(0, 0)

    @pl.when(early)
    def _():
        weight_arrived(1)

    stage_a_up_if(early)
    send_if(early & ~outer, *send_tokens(57, last_rows))
    forward(2)
    send_slots_if(~outer, 1)
    stage_a_side(2, 0)

    @pl.when(~early)
    def _():
        weight_arrived(1)

    stage_a_side(2, 1)
    send_if(early & outer, *send_tokens(57, last_rows))
    stage_a_up_if(~early)
    relay_arrived(1)
    relay_start(2)
    send_slots_if(~outer, 3)
    pair_send(1)
    stage_b(2, True)
    stage_b(0)
    forward(first)
    stage_a_side(first, 0)
    stage_a_side(first, 1)
    weight_arrived(2)
    stage_c(2)
    relay_arrived(2)
    relay_start(3)
    pair_send(2)
    stage_c(0)
    stage_d(0)
    arrived(10)
    arrived(57)
    send(11, scaled.at[2], scaled.at[3], sibling)
    forward(last)
    stage_d(2)
    stage_a_side(last, 0)
    relay_arrived(3)
    pair_send(3)
    stage_b(first, True)
    stage_a_side(last, 1)
    arrived(9)
    arrived(11)
    branch_sum((0, 1, 2), first=True)
    branch_sum((3,), last=True)
    branch_fold()
    arrived(54)
    branch_cross(0, slice(0, token_count))
    pieces = (
        cross_piece(46, 0, slice(0, capacity)),
        cross_piece(59, 0, slice(capacity, token_count)),
        cross_piece(60, 1, slice(0, token_count)),
    )
    send_if(early, *pieces[0])
    stage_c(first)
    stage_d(first)
    stage_b(last, True)
    send_if(~early, *pieces[0])
    send(*pieces[1])
    arrived(55)
    branch_cross(1, slice(0, token_count))
    send_if(early, *pieces[2])
    branch_fold_own()
    stage_c(last)
    send_if(~early, *pieces[2])
    stage_d(last)
    branch_own()

    half_own_sum = restore(0)
    half_own_sum = half_own_sum + restore(2)
    half_own_sum = half_own_sum + restore(3)
    half_own_sum = half_own_sum + restore(1)
    arrived(46)
    arrived(59)
    arrived(60)
    branch = fold_own[...] + cross_in[...].astype(F32)
    gate = 1.0 / (1.0 + jnp.exp(-branch_gate[...]))
    out[...] = (half_own_sum + gate * branch).astype(BF16)
    for copy in started.values():
        copy.wait_send()
    for hop in range(1, GROUPS):
        relay_sent(hop)
    for k in range(3):
        weight_copy(k, 0, pair_user).wait_send()

    @pl.when(c != y)
    def _():
        for k in range(3):
            weight_copy(k, 1, sibling).wait_send()


def pair_body(
    tokens,
    norm_gain,
    routing,
    route_weight,
    w_gate,
    w_up,
    w_down,
    w_branch_in,
    w_branch_out,
    branch_gate,
):
    count, quarter = tokens.shape
    ff = w_gate.shape[2]
    block = w_branch_in.shape[0]
    cap = count // 2
    half = cap // 2
    vmem = pltpu.VMEM
    rows = (GROUPS, cap, quarter)
    scratch = [
        vmem((count, quarter), BF16),
        vmem((1, quarter), F32),
        vmem((2, count), jnp.int32),
        vmem((2, count), F32),
        vmem((1, quarter), F32),
        vmem((2, quarter, ff), BF16),
        vmem((2, quarter, ff), BF16),
        vmem((2, ff, quarter), BF16),
        vmem((4, 1, count), F32),
        vmem((4, count, quarter), BF16),
        vmem((2, GROUPS, 2, block, block), BF16),
        vmem((GROUPS, cap, count), BF16),
        vmem(rows, BF16),
        vmem(rows, BF16),
        vmem(rows, BF16),
        vmem((GROUPS, 4, cap), F32),
        vmem((GROUPS, 4, cap), F32),
        vmem((GROUPS, cap, 8), F32),
        vmem((GROUPS, half, 2 * ff), BF16),
        vmem((GROUPS, half, 2 * ff), F32),
        vmem((GROUPS, half, 2 * ff), BF16),
        vmem((GROUPS, cap, ff), BF16),
        vmem(rows, BF16),
        vmem(rows, F32),
        vmem(rows, BF16),
        vmem(rows, BF16),
        vmem(rows, BF16),
        vmem((2, count, quarter), BF16),
        vmem((count, quarter), F32),
        vmem((2, count, quarter), BF16),
        vmem((count, quarter), BF16),
        vmem((count, quarter), BF16),
        vmem((count, block), BF16),
        vmem((count, block), F32),
        vmem((count, 8), F32),
        vmem((count, 8), F32),
        pltpu.SemaphoreType.DMA((10,)),
        pltpu.SemaphoreType.DMA((COPIES,)),
        pltpu.SemaphoreType.DMA((COPIES,)),
    ]
    return pl.pallas_call(
        pair_kernel,
        out_shape=pltpu.VMEM((count, quarter), BF16),
        in_specs=[pl.BlockSpec(memory_space=pltpu.HBM)] * 10,
        out_specs=pl.BlockSpec(memory_space=vmem),
        scratch_shapes=scratch,
        compiler_params=pltpu.CompilerParams(
            collective_id=0, has_side_effects=True, vmem_limit_bytes=VMEM_LIMIT
        ),
    )(
        *(
            pltpu.with_memory_space_constraint(operand, pltpu.HBM)
            for operand in (
                tokens,
                norm_gain[None, :],
                routing.T,
                route_weight.T,
                w_gate[0],
                w_up[0],
                w_down[0],
                w_branch_in,
                w_branch_out,
                branch_gate[None, :],
            )
        )
    )


def solution(mesh):
    return jax.shard_map(
        pair_body if mesh.shape["ep"] == 2 * GROUPS and mesh.shape["tp"] == 4 else body,
        mesh=mesh,
        in_specs=(
            P("ep", "tp"),
            P("tp"),
            P("ep", None),
            P("ep", None),
            P("ep", "tp", None),
            P("ep", "tp", None),
            P("ep", None, "tp"),
            P("ep", "tp"),
            P("tp", "ep"),
            P("tp"),
        ),
        out_specs=P("ep", "tp"),
        check_vma=False,
    )
```

```python
import functools

import jax
import jax.numpy as jnp
from jax import lax
from jax.experimental import pallas as pl
from jax.experimental.pallas import tpu as pltpu
from jax.sharding import PartitionSpec as P

GROUPS = 4


epsilon = 1e-06


def send_back(result):
    return lax.all_to_all(result, "ep", split_axis=0, concat_axis=0, tiled=True)


def body(
    tokens,
    norm_gain,
    routing,
    route_weight,
    w_gate,
    w_up,
    w_down,
    w_branch_in,
    w_branch_out,
    branch_gate,
):
    token_count, quarter = tokens.shape
    full_width = quarter * lax.axis_size("tp")
    floats = tokens.astype(jnp.float32)
    squares = lax.psum(jnp.sum(floats * floats, axis=1), "tp")
    normed = (floats * lax.rsqrt(squares[:, None] / full_width + epsilon) * norm_gain).astype(
        jnp.bfloat16
    )
    expert_count = lax.axis_size("ep") * w_gate.shape[0]
    capacity = token_count // (expert_count // GROUPS)
    flat_ids = routing.reshape(-1)
    one_hot = (flat_ids[:, None] == jnp.arange(expert_count, dtype=jnp.int32)[None, :]).astype(
        jnp.int32
    )
    before = jnp.cumsum(one_hot, axis=0) - one_hot
    position = flat_ids * capacity + jnp.sum(before * one_hot, axis=1)
    copies = jnp.repeat(normed, 2, axis=0)
    buffer = jnp.zeros((expert_count * capacity, quarter), jnp.bfloat16).at[position].set(copies)
    buffer = buffer.reshape(expert_count, capacity, quarter)
    gate_whole, up_whole, down_whole = (
        lax.all_gather(w_gate[0], "tp", axis=0, tiled=True),
        lax.all_gather(w_up[0], "tp", axis=0, tiled=True),
        lax.all_gather(w_down[0], "tp", axis=1, tiled=True),
    )
    row_split = lax.all_to_all(
        lax.all_to_all(buffer, "ep", split_axis=0, concat_axis=0, tiled=True),
        "tp",
        split_axis=0,
        concat_axis=2,
        tiled=True,
    )
    slot_rows = row_split.reshape(-1, row_split.shape[2])
    gate_sum = jnp.dot(slot_rows, gate_whole, preferred_element_type=jnp.float32)
    up_sum = jnp.dot(slot_rows, up_whole, preferred_element_type=jnp.float32)
    hidden = (jax.nn.silu(gate_sum) * up_sum).astype(jnp.bfloat16)
    result = jnp.dot(hidden, down_whole, preferred_element_type=jnp.float32).astype(jnp.bfloat16)
    feature_split = lax.all_to_all(
        result.reshape(row_split.shape), "tp", split_axis=2, concat_axis=0, tiled=True
    )
    returned = send_back(feature_split)
    picked = returned.reshape(expert_count * capacity, quarter)[position].reshape(
        token_count, 2, quarter
    )
    routed = jnp.sum(picked.astype(jnp.float32) * route_weight[:, :, None], axis=1)
    branch_tokens = lax.all_to_all(normed, "tp", split_axis=0, concat_axis=1, tiled=True)
    in_cols, out_rows = (
        lax.all_gather(w_branch_in, "tp", axis=1, tiled=True),
        lax.all_gather(w_branch_out, "tp", axis=0, tiled=True),
    )
    in_whole, out_whole = (
        lax.all_gather(in_cols, "ep", axis=0, tiled=True),
        lax.all_gather(out_rows, "ep", axis=1, tiled=True),
    )
    branch_hidden = jax.nn.silu(
        jnp.dot(branch_tokens, in_whole, preferred_element_type=jnp.float32)
    ).astype(jnp.bfloat16)
    branch_local = jnp.dot(branch_hidden, out_whole, preferred_element_type=jnp.float32).astype(
        jnp.bfloat16
    )
    branch = lax.all_to_all(branch_local, "tp", split_axis=1, concat_axis=0, tiled=True)
    return (routed + jax.nn.sigmoid(branch_gate) * branch.astype(jnp.float32)).astype(jnp.bfloat16)


BF16, F32 = jnp.bfloat16, jnp.float32
COPIES = 62
VMEM_LIMIT = 46 * 1024 * 1024


def dot(a, b):
    return jnp.dot(a, b, preferred_element_type=F32)


def dot_nt(a, b):
    return lax.dot_general(a, b, (((1,), (1,)), ((), ())), preferred_element_type=F32)


def silu(v):
    return v / (1.0 + jnp.exp(-v))


def pair_kernel(
    tokens_hbm,
    gain_hbm,
    routing_hbm,
    route_weight_hbm,
    w_gate,
    w_up,
    w_down,
    w_in,
    w_out,
    branch_gate_hbm,
    out,
    tokens,
    gain,
    routing,
    route_weight,
    branch_gate,
    gate_all,
    up_all,
    down_all,
    squares,
    scaled,
    branch_all,
    chosen,
    slots_out,
    slots,
    slots_s,
    scale_out,
    scale,
    scale_col,
    part_out,
    part_own,
    part_in,
    hidden,
    half_out,
    half_own,
    half_in,
    back_out,
    back,
    fold_out,
    fold_own,
    fold_in,
    cross_out,
    cross_in,
    branch_hidden,
    branch_acc,
    code_col,
    factor_col,
    load_sem,
    send_sem,
    recv_sem,
):
    ep, tp = lax.axis_index("ep"), lax.axis_index("tp")
    z, y, x, c = ep // 2, ep % 2, tp // 2, tp % 2
    token_count, quarter = tokens.shape
    ff = w_gate.shape[1]
    capacity = slots.shape[1]
    half = capacity // 2
    block = w_in.shape[0]

    def at(zz, yy, xx, cc):
        return (zz * 2 + yy, xx * 2 + cc)

    sibling = at(z, y, x, 1 - c)
    across = at(z, y, 1 - x, c)
    diagonal = at(z, y, 1 - x, 1 - c)
    pair = at(z, 1 - y, x, c)
    pair_user = at(z, 1 - y, x, y)
    pair_other = at(z, 1 - y, x, 1 - c)
    level = [z, z + 1 - 2 * (z % 2), (z + 2) % GROUPS, GROUPS - 1 - z]
    peer_of = [None] + [at(level[m], y, x, c) for m in range(1, GROUPS)]
    up = at((z + 1) % GROUPS, y, x, c)
    down = at((z + GROUPS - 1) % GROUPS, y, x, c)

    barrier = pltpu.get_barrier_semaphore()
    peers = [sibling, across, diagonal, pair, pair_other] + peer_of[1:]
    for peer in peers:
        pl.semaphore_signal(
            barrier, inc=1, device_id=peer, device_id_type=pl.DeviceIdType.MESH
        )

    loads = [
        pltpu.make_async_copy(source, target, load_sem.at[number])
        for number, (source, target) in enumerate(
            (
                (routing_hbm, routing),
                (tokens_hbm, tokens),
                (gain_hbm, gain),
                (route_weight_hbm, route_weight),
                (branch_gate_hbm, branch_gate),
                (w_in, branch_all.at[y, z, 0]),
                (w_out, branch_all.at[y, z, 1]),
            )
        )
    ]
    for load in loads:
        load.start()

    weights_of = ((w_gate, gate_all), (w_up, up_all), (w_down, down_all))

    def weight_load(k):
        source, target = weights_of[k]
        return pltpu.make_async_copy(source, target.at[c], load_sem.at[len(loads) + k])

    @pl.when(c == y)
    def _():
        for k in range(3):
            weight_load(k).start()

    loads[0].wait()
    ids = routing[0:1, :]
    group = lax.shift_right_logical(ids, 1)
    rows16 = lax.broadcasted_iota(jnp.int32, (16, token_count), 0)
    member = jnp.where(rows16 == group, 1.0, 0.0)
    earlier = jnp.where(
        lax.broadcasted_iota(jnp.int32, (token_count, token_count), 0)
        < lax.broadcasted_iota(jnp.int32, (token_count, token_count), 1),
        1.0,
        0.0,
    ).astype(BF16)
    before = dot(member.astype(BF16), earlier)
    place = jnp.sum(member * before, axis=0, keepdims=True)
    code = group.astype(F32) * capacity + place

    loads[1].wait()
    loads[2].wait()
    floats = tokens[...].astype(F32)
    scaled[0] = (floats * gain[...]).astype(BF16)
    exact = floats * floats
    high = exact.astype(BF16)
    low = (exact - high.astype(F32)).astype(BF16)
    ones = jnp.ones((16, quarter), BF16)
    squares[0] = (dot_nt(ones, high) + dot_nt(ones, low))[:1]

    slot_row = lax.broadcasted_iota(jnp.int32, (capacity, token_count), 0)

    def choose_rows(s, where, target):
        wanted = (slot_row + where * capacity).astype(F32)
        chosen[s] = jnp.where(wanted == code, 1.0, 0.0).astype(BF16)
        target[s] = dot(chosen[s], scaled[0]).astype(BF16)

    outer = (z == 0) | (z == GROUPS - 1)
    near = jnp.where(outer, 1, 2)
    choose_rows(near, jnp.where(outer, level[1], level[2]), slots_out)

    pl.semaphore_wait(barrier, len(peers))

    started = {}

    def is_own(s):
        return isinstance(s, int) and s == 0

    def key_of(number):
        return number if isinstance(number, int) else ("dynamic", len(started))

    def wait_for(number, target):
        pltpu.make_async_remote_copy(
            src_ref=target,
            dst_ref=target,
            send_sem=send_sem.at[number],
            recv_sem=recv_sem.at[number],
            device_id=sibling,
            device_id_type=pl.DeviceIdType.MESH,
        ).wait_recv()

    def send(number, source, target, device):
        copy = pltpu.make_async_remote_copy(
            src_ref=source,
            dst_ref=target,
            send_sem=send_sem.at[number],
            recv_sem=recv_sem.at[number],
            device_id=device,
            device_id_type=pl.DeviceIdType.MESH,
        )
        copy.start()
        started[key_of(number)] = copy

    def send_if(condition, number, source, target, device):
        copy = pltpu.make_async_remote_copy(
            src_ref=source,
            dst_ref=target,
            send_sem=send_sem.at[number],
            recv_sem=recv_sem.at[number],
            device_id=device,
            device_id_type=pl.DeviceIdType.MESH,
        )

        @pl.when(condition)
        def _():
            copy.start()

        started[number] = copy

    def arrived(number):
        started[number].wait_recv()

    def weight_copy(k, sem, device):
        source, target = weights_of[k]
        return pltpu.make_async_remote_copy(
            src_ref=source,
            dst_ref=target.at[c],
            send_sem=send_sem.at[2 * k + sem],
            recv_sem=recv_sem.at[2 * k + c],
            device_id=device,
            device_id_type=pl.DeviceIdType.MESH,
        )

    def send_slots(s):
        send(19 + s, slots_out.at[s], slots.at[s], peer_of[s])

    def send_slots_if(condition, s):
        send_if(condition, 19 + s, slots_out.at[s], slots.at[s], peer_of[s])

    def send_scale(s):
        send(22 + s, scale_out.at[s], scale.at[s], peer_of[s])

    def relay(hop, upward):
        number = (12 if upward else 47) + hop - 1
        held = z - (hop - 1) if upward else z + (hop - 1)
        came = z - hop if upward else z + hop
        held, came = (held + GROUPS) % GROUPS, (came + GROUPS) % GROUPS
        sends = (z <= GROUPS - 2) & (z >= hop - 1)
        gets = z >= hop
        if not upward:
            sends = (z >= 1) & (z <= GROUPS - hop)
            gets = z <= GROUPS - 1 - hop

        def copy(row):
            return pltpu.make_async_remote_copy(
                src_ref=branch_all.at[y, row],
                dst_ref=branch_all.at[y, row],
                send_sem=send_sem.at[number],
                recv_sem=recv_sem.at[number],
                device_id=up if upward else down,
                device_id_type=pl.DeviceIdType.MESH,
            )

        return sends, gets, lambda: copy(held), lambda: copy(came)

    def relay_start(hop):
        for upward in (True, False):
            sends, _, outgoing, _ = relay(hop, upward)

            @pl.when(sends)
            def _():
                outgoing().start()

    def relay_arrived(hop):
        for upward in (True, False):
            _, gets, _, incoming = relay(hop, upward)

            @pl.when(gets)
            def _():
                incoming().wait_recv()

    def relay_sent(hop):
        for upward in (True, False):
            sends, _, outgoing, _ = relay(hop, upward)

            @pl.when(sends)
            def _():
                outgoing().wait_send()

    send(7, squares.at[0], squares.at[2], across)
    send(8, squares.at[0], squares.at[3], diagonal)
    send(6, squares.at[0], squares.at[1], sibling)
    early = c == y
    send_slots_if(outer, 1)
    send_slots_if(~outer, 2)
    part_rows = token_count // 2
    first_rows, last_rows = pl.ds(0, part_rows), pl.ds(part_rows, part_rows)

    def send_tokens(number, rows):
        return number, scaled.at[0, rows], scaled.at[2, rows], across

    send(*send_tokens(10, first_rows))
    send_if(~early, *send_tokens(57, last_rows))
    for k in range(3):
        weight_copy(k, 0, pair_user).start()

    @pl.when(c != y)
    def _():
        for k in range(3):
            weight_copy(k, 1, sibling).start()

    choose_rows(3 - near, jnp.where(outer, level[2], level[1]), slots_out)
    send_slots_if(outer, 2)
    loads[5].wait()
    loads[6].wait()
    relay_start(1)
    send(9, scaled.at[0], scaled.at[1], sibling)

    def weight_arrived(k):
        source, target = weights_of[k]

        def wait(h):
            pltpu.make_async_remote_copy(
                src_ref=source,
                dst_ref=target.at[h],
                send_sem=send_sem.at[2 * k],
                recv_sem=recv_sem.at[2 * k + h],
                device_id=sibling,
                device_id_type=pl.DeviceIdType.MESH,
            ).wait_recv()

        wait(1 - c)

        @pl.when(c != y)
        def _():
            wait(c)

        @pl.when(c == y)
        def _():
            weight_load(k).wait()

    def pair_send(m):
        rows = branch_all.at[y, level[m]]
        send(15 + m, rows, rows, pair)

    choose_rows(0, level[0], slots)
    send(26, slots.at[0], slots_s.at[0], sibling)
    choose_rows(3, level[3], slots_out)
    pair_send(0)

    loads[3].wait()
    loads[4].wait()
    first, second = route_weight[0:1, :], route_weight[1:2, :]
    even_first = (ids & 1) == 0
    for_even = jnp.where(even_first, first, second)
    for_odd = jnp.where(even_first, second, first)
    for number in (6, 7, 8):
        arrived(number)
    total = squares[0] + squares[1] + squares[2] + squares[3]
    factor = lax.rsqrt(total / (4 * quarter) + epsilon)
    factor_col[...] = jnp.transpose(jnp.broadcast_to(factor, (8, token_count)))
    code_col[...] = jnp.transpose(jnp.broadcast_to(code, (8, token_count)))
    weights = jnp.where(
        rows16 == 0, for_even, jnp.where(rows16 == 1, for_odd, factor)
    )
    weights_high = weights.astype(BF16)
    weights_low = (weights - weights_high.astype(F32)).astype(BF16)
    for s in (2, 3, 1, 0):
        slot_weights = (dot_nt(weights_high, chosen[s]) + dot_nt(weights_low, chosen[s]))[:4]
        if s == 0:
            scale[0] = slot_weights
        else:
            scale_out[s] = slot_weights
            send_scale(s)
    send_slots_if(outer, 3)

    def project(s, start, weights):
        own = slots[s, pl.ds(start, half), :]
        other = slots_s[s, pl.ds(start, half), :]
        return dot(own, weights[c]) + dot(other, weights[1 - c])

    mine = pl.multiple_of(x * half, half)
    theirs = pl.multiple_of((1 - x) * half, half)

    def forward(s):
        wait_for(19 + s, slots.at[s])
        send(26 + s, slots.at[s], slots_s.at[s], sibling)

    sides = (slice(0, ff), slice(ff, 2 * ff))

    def stage_a(s):
        wait_for(26 + s, slots_s.at[s])
        for side, weights in zip(sides, (gate_all, up_all)):
            part_out[s, :, side] = project(s, theirs, weights).astype(BF16)
        send(30 + s, part_out.at[s], part_in.at[s], across)
        for side, weights in zip(sides, (gate_all, up_all)):
            part_own[s, :, side] = project(s, mine, weights)

    def stage_a_up_if(condition):
        number, side = 50, sides[1]
        copy = pltpu.make_async_remote_copy(
            src_ref=part_out.at[0, :, side],
            dst_ref=part_in.at[0, :, side],
            send_sem=send_sem.at[number],
            recv_sem=recv_sem.at[number],
            device_id=across,
            device_id_type=pl.DeviceIdType.MESH,
        )
        started[number] = copy

        @pl.when(condition)
        def _():
            part_out[0, :, side] = project(0, theirs, up_all).astype(BF16)
            copy.start()
            part_own[0, :, side] = project(0, mine, up_all)

    def stage_a_side(s, k):
        if k == 0:
            wait_for(26 + s, slots_s.at[s])
        side, weights = sides[k], (gate_all, up_all)[k]
        part_out[s, :, side] = project(s, theirs, weights).astype(BF16)
        number = 30 + s if k == 0 else 50 + s
        send(number, part_out.at[s, :, side], part_in.at[s, :, side], across)
        part_own[s, :, side] = project(s, mine, weights)

    def stage_b(s, sided=False):
        if not is_own(s):
            wait_for(22 + s, scale.at[s])
        scale_col[s] = jnp.transpose(jnp.concatenate([scale[s], scale[s]], axis=0))
        if is_own(s) or sided:
            wait_for(30 + s, part_in.at[s, :, sides[0]])
            wait_for(50 + s, part_in.at[s, :, sides[1]])
        else:
            wait_for(30 + s, part_in.at[s])
        rescale = scale_col[s, pl.ds(mine, half), 2:3]
        gate_sum = (part_own[s, :, :ff] + part_in[s, :, :ff].astype(F32)) * rescale
        up_sum = (part_own[s, :, ff:] + part_in[s, :, ff:].astype(F32)) * rescale
        hidden[s, pl.ds(mine, half), :] = (silu(gate_sum) * up_sum).astype(BF16)
        kept = hidden.at[s, pl.ds(mine, half), :]
        send(34 + s, kept, kept, across)

    def stage_c(s):
        wait_for(34 + s, hidden.at[s, pl.ds(theirs, half), :])
        weight = jnp.where(c == 0, scale_col[s, :, 0:1], scale_col[s, :, 1:2])
        units = hidden[s]
        half_out[s] = (dot(units, down_all[1 - c]) * weight).astype(BF16)
        send(38 + s, half_out.at[s], half_in.at[s], sibling)
        half_own[s] = dot(units, down_all[c]) * weight

    def stage_d(s):
        wait_for(38 + s, half_in.at[s])
        both = (half_own[s] + half_in[s].astype(F32)).astype(BF16)
        if is_own(s):
            back[0] = both
        else:
            back_out[s] = both
            zone = level[s] if isinstance(s, int) else jnp.where(s == 1, level[1], level[3])
            send(41 + s, back_out.at[s], back.at[s], at(zone, y, x, c))

    quarters = (tp, x * 2 + 1 - c, (1 - x) * 2 + c, (1 - x) * 2 + 1 - c)

    def branch_sum(members, first=False, last=False):
        sums = jnp.zeros((token_count, block), F32) if first else branch_acc[...]
        for m in members:
            wait_for(15 + m, branch_all.at[1 - y, level[m]])
            q = level[m]
            k = (x + q // 2) % 2 * 2 + (c + q) % 2
            sums = sums + dot(scaled[k, :, :block], branch_all[0, q, 0])
            sums = sums + dot(scaled[k, :, block:], branch_all[1, q, 0])
        if last:
            branch_hidden[...] = silu(sums * factor_col[:, 0:1]).astype(BF16)
        else:
            branch_acc[...] = sums

    def branch_part(q, side):
        return dot(branch_hidden[...], branch_all[side, q, 1])

    left, right = slice(0, block), slice(block, 2 * block)

    def branch_fold():
        for number, side, columns in ((54, 0, left), (55, 1, right)):
            fold_out[1, :, columns] = branch_part(quarters[3], side).astype(BF16)
            send(number, fold_out.at[1, :, columns], fold_in.at[1, :, columns], sibling)

    def branch_fold_own():
        for side, columns in ((0, left), (1, right)):
            fold_out[0, :, columns] = branch_part(quarters[1], side).astype(BF16)
        send(58, fold_out.at[0], fold_in.at[0], sibling)

    def branch_cross(side, rows):
        columns = (left, right)[side]
        cross_out[rows, columns] = (
            dot(branch_hidden[rows], branch_all[side, quarters[2], 1])
            + fold_in[1, rows, columns].astype(F32)
        ).astype(BF16)

    def cross_piece(number, side, rows):
        columns = (left, right)[side]
        return number, cross_out.at[rows, columns], cross_in.at[rows, columns], across

    def branch_own():
        arrived(58)
        for side in range(2):
            columns = slice(side * block, (side + 1) * block)
            fold_own[:, columns] = branch_part(quarters[0], side) + fold_in[
                0, :, columns
            ].astype(F32)

    slot_lane = lax.broadcasted_iota(jnp.int32, (token_count, capacity), 1)

    def restore(s):
        if s:
            wait_for(41 + s, back.at[s])
        wanted = (slot_lane + level[s] * capacity).astype(F32)
        choose = jnp.where(wanted == code_col[:, 0:1], 1.0, 0.0).astype(BF16)
        return dot(choose, back[s])

    first = jnp.where(outer, 3, 1)
    last = 4 - first
    weight_arrived(0)
    stage_a_side(0, 0)

    @pl.when(early)
    def _():
        weight_arrived(1)

    stage_a_up_if(early)
    send_if(early & ~outer, *send_tokens(57, last_rows))
    forward(2)
    send_slots_if(~outer, 1)
    stage_a_side(2, 0)

    @pl.when(~early)
    def _():
        weight_arrived(1)

    stage_a_side(2, 1)
    send_if(early & outer, *send_tokens(57, last_rows))
    stage_a_up_if(~early)
    relay_arrived(1)
    relay_start(2)
    send_slots_if(~outer, 3)
    pair_send(1)
    stage_b(2, True)
    stage_b(0)
    forward(first)
    stage_a_side(first, 0)
    stage_a_side(first, 1)
    weight_arrived(2)
    stage_c(2)
    relay_arrived(2)
    relay_start(3)
    pair_send(2)
    stage_c(0)
    stage_d(0)
    arrived(10)
    arrived(57)
    send(11, scaled.at[2], scaled.at[3], sibling)
    forward(last)
    stage_d(2)
    stage_a_side(last, 0)
    relay_arrived(3)
    pair_send(3)
    stage_b(first, True)
    stage_a_side(last, 1)
    arrived(9)
    arrived(11)
    branch_sum((0, 1, 2), first=True)
    branch_sum((3,), last=True)
    branch_fold()
    arrived(54)
    branch_cross(0, slice(0, token_count))
    pieces = (
        cross_piece(46, 0, slice(0, capacity)),
        cross_piece(59, 0, slice(capacity, token_count)),
        cross_piece(60, 1, slice(0, capacity)),
        cross_piece(61, 1, slice(capacity, token_count)),
    )
    send_if(early, *pieces[0])
    stage_c(first)
    stage_d(first)
    stage_b(last, True)
    send_if(~early, *pieces[0])
    send(*pieces[1])
    arrived(55)
    branch_cross(1, slice(0, token_count))
    send(*pieces[2])
    send_if(early, *pieces[3])
    branch_fold_own()
    stage_c(last)
    send_if(~early, *pieces[3])
    stage_d(last)
    branch_own()

    half_own_sum = restore(0)
    half_own_sum = half_own_sum + restore(2)
    half_own_sum = half_own_sum + restore(3)
    half_own_sum = half_own_sum + restore(1)
    arrived(46)
    arrived(59)
    arrived(60)
    arrived(61)
    branch = fold_own[...] + cross_in[...].astype(F32)
    gate = 1.0 / (1.0 + jnp.exp(-branch_gate[...]))
    out[...] = (half_own_sum + gate * branch).astype(BF16)
    for copy in started.values():
        copy.wait_send()
    for hop in range(1, GROUPS):
        relay_sent(hop)
    for k in range(3):
        weight_copy(k, 0, pair_user).wait_send()

    @pl.when(c != y)
    def _():
        for k in range(3):
            weight_copy(k, 1, sibling).wait_send()


def pair_body(
    tokens,
    norm_gain,
    routing,
    route_weight,
    w_gate,
    w_up,
    w_down,
    w_branch_in,
    w_branch_out,
    branch_gate,
):
    count, quarter = tokens.shape
    ff = w_gate.shape[2]
    block = w_branch_in.shape[0]
    cap = count // 2
    half = cap // 2
    vmem = pltpu.VMEM
    rows = (GROUPS, cap, quarter)
    scratch = [
        vmem((count, quarter), BF16),
        vmem((1, quarter), F32),
        vmem((2, count), jnp.int32),
        vmem((2, count), F32),
        vmem((1, quarter), F32),
        vmem((2, quarter, ff), BF16),
        vmem((2, quarter, ff), BF16),
        vmem((2, ff, quarter), BF16),
        vmem((4, 1, count), F32),
        vmem((4, count, quarter), BF16),
        vmem((2, GROUPS, 2, block, block), BF16),
        vmem((GROUPS, cap, count), BF16),
        vmem(rows, BF16),
        vmem(rows, BF16),
        vmem(rows, BF16),
        vmem((GROUPS, 4, cap), F32),
        vmem((GROUPS, 4, cap), F32),
        vmem((GROUPS, cap, 8), F32),
        vmem((GROUPS, half, 2 * ff), BF16),
        vmem((GROUPS, half, 2 * ff), F32),
        vmem((GROUPS, half, 2 * ff), BF16),
        vmem((GROUPS, cap, ff), BF16),
        vmem(rows, BF16),
        vmem(rows, F32),
        vmem(rows, BF16),
        vmem(rows, BF16),
        vmem(rows, BF16),
        vmem((2, count, quarter), BF16),
        vmem((count, quarter), F32),
        vmem((2, count, quarter), BF16),
        vmem((count, quarter), BF16),
        vmem((count, quarter), BF16),
        vmem((count, block), BF16),
        vmem((count, block), F32),
        vmem((count, 8), F32),
        vmem((count, 8), F32),
        pltpu.SemaphoreType.DMA((10,)),
        pltpu.SemaphoreType.DMA((COPIES,)),
        pltpu.SemaphoreType.DMA((COPIES,)),
    ]
    return pl.pallas_call(
        pair_kernel,
        out_shape=pltpu.VMEM((count, quarter), BF16),
        in_specs=[pl.BlockSpec(memory_space=pltpu.HBM)] * 10,
        out_specs=pl.BlockSpec(memory_space=vmem),
        scratch_shapes=scratch,
        compiler_params=pltpu.CompilerParams(
            collective_id=0, has_side_effects=True, vmem_limit_bytes=VMEM_LIMIT
        ),
    )(
        *(
            pltpu.with_memory_space_constraint(operand, pltpu.HBM)
            for operand in (
                tokens,
                norm_gain[None, :],
                routing.T,
                route_weight.T,
                w_gate[0],
                w_up[0],
                w_down[0],
                w_branch_in,
                w_branch_out,
                branch_gate[None, :],
            )
        )
    )


def solution(mesh):
    return jax.shard_map(
        pair_body if mesh.shape["ep"] == 2 * GROUPS and mesh.shape["tp"] == 4 else body,
        mesh=mesh,
        in_specs=(
            P("ep", "tp"),
            P("tp"),
            P("ep", None),
            P("ep", None),
            P("ep", "tp", None),
            P("ep", "tp", None),
            P("ep", None, "tp"),
            P("ep", "tp"),
            P("tp", "ep"),
            P("tp"),
        ),
        out_specs=P("ep", "tp"),
        check_vma=False,
    )
```
